256 devices in a mesh: ep: 16 (over y, x), tp: 16 (over z, core).
Axes of the slice: x: 4, y: 4, z: 8, core: 2. Of those that a mesh axis runs over, the one named last changes fastest.
Arguments:
- mixer_input_channels: bfloat16 [32768, 2048], P('ep', 'tp'), may hold values from -6 to 6
- output_gate_logits: bfloat16 [32768, 2048], P('ep', 'tp'), may hold values from -6 to 6
- head_group_input_map: bfloat16 [32768, 256], P('ep'), may hold values from -6 to 6
- head_group_output_map: bfloat16 [32768, 256], P('ep'), may hold values from -6 to 6
- input_channel_taps: bfloat16 [4, 2048], P(None, 'tp'), may hold values from -3 to 3
- input_map_taps: bfloat16 [4, 256], replicated, may hold values from -3 to 3
- output_map_taps: bfloat16 [4, 256], replicated, may hold values from -3 to 3
- step_logits: float32 [32, 32768], P('tp', 'ep'), may hold values from -5 to 5
- head_log_rate: float32 [32], P('tp'), may hold values from -20 to -2
- extra_log_decay: float32 [32, 32768], P('tp', 'ep'), may hold values from -1 to 0
- head_direct_scale: float32 [32], P('tp'), may hold values from 1 to 6
- gated_norm_scale: bfloat16 [2048], P('tp'), may hold values from 0.099609375 to 1.8984375
- mixer_output_weight: bfloat16 [2048, 2048], P('tp'), may hold values from -0.125 to 0.125
- second_batch_tokens: bfloat16 [4096, 2048], P('ep'), may hold values from -6 to 6
- pre_expert_norm_scale: bfloat16 [2048], replicated, may hold values from 0.099609375 to 1.8984375
- group_router_columns: bfloat16 [2048, 4], replicated
- expert_router_columns: bfloat16 [2048, 16], replicated
- routes: int32 [4096, 2], P('ep'), may hold values from 0 to 15, all different within a row; in each aligned block of 256 rows (0 to 255, 256 to 511, ...) at most 64 rows name the same one
- expert_gate_weight: bfloat16 [16, 2048, 4096], P('ep', None, 'tp'), may hold values from -0.125 to 0.125
- expert_up_weight: bfloat16 [16, 2048, 4096], P('ep', None, 'tp'), may hold values from -0.125 to 0.125
- expert_down_weight: bfloat16 [16, 4096, 2048], P('ep', 'tp'), may hold values from -0.125 to 0.125
Outputs:
- mixer_out: bfloat16 [32768, 2048], P(('ep', 'tp'))
- experts_out: bfloat16 [4096, 2048], P('ep', 'tp')
The draws below stay inside these ranges and needn't reach their ends.
Inputs may be any that keep to these rules, and one draw needn't show every extreme that they name: `routes`: in each aligned block of 256 rows no expert is named more than 64 times, some expert exactly 64 times in some block; a row's two experts differ.
All inputs are finite; a program needn't handle non-finite values.
Results may differ from the reference program's by a relative error of at most 0.019.
Values may be sent and summed in bfloat16 or wider, within the bound.
A program may use at most 128 MiB of HBM per device.

```python
import math
import jax
import jax.numpy as jnp
import numpy as np
from jax import lax

D = 2048
HEADS = 32
HEAD_DIM = 64
STATE = 64
GROUPS = 4
CONV = 4
BLOCK = 128
FF = 4096
TOK_SHARD = 2048
TOKB = 256
INNER = 2048
SEQ = 32768
TOKENS = 4096
EXPERTS = 16
EXPERT_GROUPS = 4
CAP = 64
FF_SHARD = 256
N_EP = 16
N_TP = 16


def draw_step_logits(key, part):
    first, second = jax.random.split(jax.random.fold_in(key, 11))
    span = max(TOK_SHARD // 2, 1)
    offset = jax.random.uniform(second, (HEADS, SEQ // span), jnp.float32, -1.5, 1.5)
    offset = jnp.repeat(offset, span, axis=1)
    noise = jnp.clip(jax.random.normal(first, (HEADS, SEQ), jnp.float32), -3.0, 3.0)
    return (noise + offset).astype(jnp.float32)


def draw_head_log_rate(key, part):
    first, second, third = jax.random.split(jax.random.fold_in(key, 12), 3)
    share = 0.5
    quick = jax.random.uniform(first, (HEADS,), jnp.float32) < share
    quick_rate = jax.random.uniform(second, (HEADS,), jnp.float32, math.log(0.02), math.log(0.1))
    slow_rate = jax.random.uniform(third, (HEADS,), jnp.float32, math.log(0.3), math.log(2.3)) - math.log(SEQ)
    return jnp.where(quick, quick_rate, slow_rate).astype(jnp.float32)


def draw_extra_log_decay(key, part):
    first, second = jax.random.split(jax.random.fold_in(key, 13))
    struck = jax.random.uniform(first, (HEADS, SEQ), jnp.float32) < 6.0 / SEQ
    depth = jax.random.uniform(second, (HEADS, SEQ), jnp.float32, math.log(0.5), math.log(0.8))
    return jnp.where(struck, depth, 0.0).astype(jnp.float32)


def router_columns(key, columns):
    first = jax.random.fold_in(key, 0)
    base = jax.random.normal(first, (D, columns), jnp.float32) / math.sqrt(D)
    return base.astype(jnp.bfloat16)


def draw_group_router_columns(key, part):
    return router_columns(jax.random.fold_in(key, 14), EXPERT_GROUPS)


def draw_expert_router_columns(key, part):
    return router_columns(jax.random.fold_in(key, 15), EXPERTS)


def spiked(result, stream_key, source, target, shards_of, factor):
    owner, partner = [(jnp.arange(result.shape[position]) // (result.shape[position] // shards_of)).reshape([-1 if axis == position else 1 for axis in range(result.ndim)]) for position in (source, target)]
    chosen = jax.random.permutation(stream_key, shards_of)[partner]
    strong = (owner == chosen) | (owner == (partner + shards_of // 2) % shards_of)
    return jnp.where(strong, factor * result, result)


def block_levels(stream_key, extent, cuts, low, high):
    def one(axis_at, blocks):
        draws = jax.random.uniform(jax.random.fold_in(jax.random.fold_in(stream_key, 6), axis_at), (blocks,), jnp.float32, low / len(cuts), high / len(cuts))
        return jnp.repeat(jnp.exp(draws), extent[axis_at] // blocks).reshape((-1,) + (1,) * (len(extent) - axis_at - 1))

    gain = one(*cuts[0])
    for cut in cuts[1:]:
        gain = gain * one(*cut)
    return gain


def deal_out(stream_key, own, number, rows, amount, top, bound, skew):
    order = jax.random.permutation(stream_key, amount)
    packed, common = load_shares(amount, rows * top, bound, skew, True), load_shares(amount, rows * top, bound, skew, False)
    places = jnp.arange(amount)

    def named(sizes, turn):
        used = int((sizes > 0).sum())
        fixed = max(1, used // 4)
        moved = fixed + (places - fixed + turn * (used - fixed)) % max(1, amount - fixed)
        return jnp.zeros((amount,), jnp.int32).at[order[jnp.where(places < fixed, places, moved)]].set(jnp.asarray(sizes, jnp.int32))

    sizes = jnp.where(number % 4 == 0, named(packed, number // 4), named(common, number - number // 4 - 1))
    mixed = jax.random.permutation(jax.random.fold_in(own, 3), amount)
    donor, taker = mixed[0:amount // 2 * 2:2], mixed[1:amount // 2 * 2:2]
    margin = jnp.minimum(sizes[donor] - 1, bound - sizes[taker]) // 2
    margin = jnp.where((donor == order[0]) | (taker == order[0]) | (sizes[taker] == 0), 0, jnp.maximum(margin, 0))
    moved = jax.random.randint(jax.random.fold_in(own, 4), (amount // 2,), 0, 1 << 20) % (margin + 1)
    sizes = sizes.at[donor].add(-moved).at[taker].add(moved)
    members = jnp.searchsorted(jnp.cumsum(sizes), jnp.arange(rows * top), side="right").astype(jnp.int32)
    grid = members.reshape(top, rows).T
    grid = grid[jax.random.permutation(jax.random.fold_in(own, 1), rows)]
    turn = jax.random.randint(jax.random.fold_in(own, 2), (rows, 1), 0, top)
    return jnp.take_along_axis(grid, (jnp.arange(top)[None, :] + turn) % top, axis=1)


def load_shares(number_of, total, limit, skew, full):
    loads = [(1 << 20) // math.isqrt(rank ** skew) + 1 for rank in range(1, number_of + 1)]
    largest = limit if full else min(limit, max(-(-total // number_of), total * loads[0] // sum(loads)))
    least = 1 if total - largest >= number_of - 1 else 0
    given, spare = [largest] + [least] * (number_of - 1), total - largest - least * (number_of - 1)
    while spare > 0:
        free = [i for i in range(1, number_of) if given[i] < largest] or [i for i in range(1, number_of) if given[i] < limit]
        whole, left = sum([loads[i] for i in free]), spare
        for i in free:
            more = min(limit - given[i], max(1, left * loads[i] // whole), spare)
            given[i] = given[i] + more
            spare = spare - more
    return np.array(given)


def bell_draw(key, shape, spread, most, cuts=(), kind=jnp.bfloat16):
    entries = jax.random.normal(key, shape, jnp.float32) * spread
    if len(cuts) > 0:
        entries = block_levels(key, shape, cuts, -0.22, 0.18) * entries
    return jnp.clip(entries, min=-most, max=most).astype(kind)


def noise_with(key, extent, deviation, reach, shards, heavy, kind=jnp.bfloat16):
    result = deviation * jax.random.normal(key, extent, jnp.float32)
    if shards:
        result = result * block_levels(key, extent, shards, -0.22, 0.18)
    return jnp.clip(spiked(result, jax.random.fold_in(key, 3), *heavy), -reach, reach).astype(kind)


def setup_inputs(seed: int = 0) -> dict:
    splits = jax.random.split(jax.random.key(seed), 22)
    mixer_input_channels = bell_draw(splits[0], (SEQ, INNER), 1.0, 6.0, ((0, 16), (1, 16)))
    output_gate_logits = bell_draw(splits[1], (SEQ, INNER), 1.0, 6.0, ((0, 16), (1, 16)))
    head_group_input_map = bell_draw(splits[2], (SEQ, GROUPS * STATE), 1.0, 6.0, ((0, 16),))
    head_group_output_map = bell_draw(splits[3], (SEQ, GROUPS * STATE), 1.0, 6.0, ((0, 16),))
    input_channel_taps = bell_draw(splits[4], (CONV, INNER), CONV ** -0.5, 3.0, ((1, 16),))
    input_map_taps = bell_draw(splits[5], (CONV, GROUPS * STATE), CONV ** -0.5, 3.0)
    output_map_taps = bell_draw(splits[6], (CONV, GROUPS * STATE), CONV ** -0.5, 3.0)
    step_logits = draw_step_logits(jax.random.fold_in(splits[21], 71), 0)
    head_log_rate = draw_head_log_rate(jax.random.fold_in(splits[21], 71), 0)
    extra_log_decay = draw_extra_log_decay(jax.random.fold_in(splits[21], 71), 0)
    head_direct_scale = jnp.clip(1.0 + 5.0 * jax.random.uniform(splits[10], (HEADS,), jnp.float32) ** block_levels(splits[10], (HEADS,), ((0, 16),), -0.2, 0.2), 1.0, 6.0)
    gated_norm_scale = jnp.clip(1.0 + 0.18 * jax.random.normal(splits[11], (INNER,), jnp.float32), 0.099609375, 1.8984375).astype(jnp.bfloat16)
    mixer_output_weight = bell_draw(splits[12], (INNER, D), INNER ** -0.5, 0.125, ((0, 16),))
    second_batch_tokens = bell_draw(splits[13], (TOKENS, D), 1.0, 6.0, ((0, 16),))
    pre_expert_norm_scale = jnp.clip(1.0 + 0.18 * jax.random.normal(splits[14], (D,), jnp.float32), 0.099609375, 1.8984375).astype(jnp.bfloat16)
    group_router_columns = draw_group_router_columns(jax.random.fold_in(splits[21], 71), 0)
    expert_router_columns = draw_expert_router_columns(jax.random.fold_in(splits[21], 71), 0)
    routes_keys = jax.random.split(jax.random.fold_in(splits[17], 1), TOKENS // TOKB)
    routes_turns = jax.random.permutation(jax.random.fold_in(splits[17], 3), TOKENS // TOKB)
    routes = jax.vmap(lambda own, number: deal_out(jax.random.fold_in(splits[17], 2), own, number, TOKB, EXPERTS, 2, CAP, 2))(routes_keys, routes_turns).reshape((TOKENS, 2))
    expert_gate_weight = bell_draw(splits[18], (EXPERTS, D, FF), D ** -0.5, 0.125, ((0, 16), (2, 16)))
    expert_up_weight = bell_draw(splits[19], (EXPERTS, D, FF), D ** -0.5, 0.125, ((0, 16), (2, 16)))
    expert_down_weight = noise_with(splits[20], (EXPERTS, FF, D), FF ** -0.5, 0.125, ((0, 16), (1, 16)), (1, 2, 16, 2.0))
    return {"mixer_input_channels": mixer_input_channels, "output_gate_logits": output_gate_logits, "head_group_input_map": head_group_input_map, "head_group_output_map": head_group_output_map, "input_channel_taps": input_channel_taps, "input_map_taps": input_map_taps, "output_map_taps": output_map_taps, "step_logits": step_logits, "head_log_rate": head_log_rate, "extra_log_decay": extra_log_decay, "head_direct_scale": head_direct_scale, "gated_norm_scale": gated_norm_scale, "mixer_output_weight": mixer_output_weight, "second_batch_tokens": second_batch_tokens, "pre_expert_norm_scale": pre_expert_norm_scale, "group_router_columns": group_router_columns, "expert_router_columns": expert_router_columns, "routes": routes, "expert_gate_weight": expert_gate_weight, "expert_up_weight": expert_up_weight, "expert_down_weight": expert_down_weight}


eps = 1e-06
exact_prec = lax.Precision.HIGHEST

def causal_conv(joined, taps):
    width = taps.shape[0]
    length = joined.shape[0]
    padded = jnp.pad(joined.astype(jnp.float32), ((width - 1, 0), (0, 0)))
    total = jnp.zeros((length, joined.shape[1]), jnp.float32)
    for j in range(width):
        total = total + taps[j].astype(jnp.float32) * padded[j:j + length]
    return jax.nn.silu(total).astype(jnp.bfloat16)

def slot_positions(route_rows, n_experts):
    flat = route_rows.reshape(-1)
    onehot = (flat[:, None] == jnp.arange(n_experts, dtype=jnp.int32)[None, :]).astype(jnp.int32)
    return (lax.optimization_barrier(jnp.sum(onehot * jnp.cumsum(onehot, axis=0), axis=1)) - 1).astype(jnp.int32)

def route_weights(group_logits, expert_logits, routes):
    n_groups = group_logits.shape[1]
    n_experts = expert_logits.shape[1]
    per_group = n_experts // n_groups
    group_lp = jax.nn.log_softmax(group_logits, axis=-1)
    inner_lp = jax.nn.log_softmax(expert_logits.reshape(-1, n_groups, per_group), axis=-1).reshape(-1, n_experts)
    total = jnp.repeat(group_lp, per_group, axis=1) + inner_lp
    pick = routes[:, :, None] == jnp.arange(n_experts, dtype=jnp.int32)[None, None, :]
    chosen = lax.optimization_barrier(jnp.sum(jnp.where(pick, total[:, None, :], 0.0), axis=-1))
    return jax.nn.softmax(chosen, axis=-1)

def expert_apply(items):
    rows, gate_w, up_w, down_w = items
    gate = jnp.dot(rows, gate_w, preferred_element_type=jnp.float32)
    upper = jnp.dot(rows, up_w, preferred_element_type=jnp.float32)
    hidden = (jax.nn.silu(gate) * upper).astype(jnp.bfloat16)
    parts = hidden.reshape(rows.shape[0], N_TP, FF_SHARD).astype(jnp.float32)
    down_parts = down_w.reshape(N_TP, FF_SHARD, D).astype(jnp.float32)
    partial_sums = jnp.einsum('rjf,jfd->jrd', parts, down_parts).astype(jnp.bfloat16)
    return lax.optimization_barrier(jnp.sum(partial_sums.astype(jnp.float32), axis=0)).astype(jnp.bfloat16)

def reference(mixer_input_channels, output_gate_logits, head_group_input_map, head_group_output_map, input_channel_taps, input_map_taps, output_map_taps, step_logits, head_log_rate, extra_log_decay, head_direct_scale, gated_norm_scale, mixer_output_weight, second_batch_tokens, pre_expert_norm_scale, group_router_columns, expert_router_columns, routes, expert_gate_weight, expert_up_weight, expert_down_weight):
    joined = jnp.concatenate([mixer_input_channels, head_group_input_map, head_group_output_map], axis=1)
    taps = jnp.concatenate([input_channel_taps, input_map_taps, output_map_taps], axis=1)
    conv = causal_conv(joined, taps)
    xs = conv[:, :INNER]
    bs = conv[:, INNER:INNER + GROUPS * STATE]
    cs = conv[:, INNER + GROUPS * STATE:]
    time_step = jax.nn.softplus(step_logits)
    position_log_decay = extra_log_decay - time_step * jnp.exp(head_log_rate)[:, None]
    per_group = HEADS // GROUPS
    xs_f = xs.astype(jnp.float32).reshape(SEQ, HEADS, HEAD_DIM)
    x_dt = xs_f * jnp.transpose(time_step)[:, :, None]
    bs_h = jnp.repeat(bs.astype(jnp.float32).reshape(SEQ, GROUPS, STATE), per_group, axis=1)
    cs_h = jnp.repeat(cs.astype(jnp.float32).reshape(SEQ, GROUPS, STATE), per_group, axis=1)
    nblk = SEQ // BLOCK
    items = (x_dt.reshape(nblk, BLOCK, HEADS, HEAD_DIM), bs_h.reshape(nblk, BLOCK, HEADS, STATE), cs_h.reshape(nblk, BLOCK, HEADS, STATE), jnp.transpose(position_log_decay).reshape(nblk, BLOCK, HEADS))
    lower = jnp.tril(jnp.ones((BLOCK, BLOCK), bool))[:, :, None]

    def one_block(state, item):
        xb, bb, cb, lb = item
        cum = jnp.cumsum(lb, axis=0)
        diff = cum[:, None, :] - cum[None, :, :]
        weight = jnp.where(lower, jnp.exp(jnp.where(lower, diff, 0.0)), 0.0)
        scores = jnp.einsum('lhn,shn->lsh', cb, bb, precision=exact_prec)
        inner = jnp.einsum('lsh,shp->lhp', scores * weight, xb, precision=exact_prec)
        carried = jnp.einsum('lhn,hpn->lhp', cb, state, precision=exact_prec) * jnp.exp(cum)[:, :, None]
        tail = jnp.exp(cum[-1:] - cum)
        new_state = state * jnp.exp(cum[-1])[:, None, None] + jnp.einsum('shp,shn->hpn', xb * tail[:, :, None], bb, precision=exact_prec)
        return (new_state, inner + carried)
    start = jnp.zeros((HEADS, HEAD_DIM, STATE), jnp.float32)
    _, ssm = lax.scan(one_block, start, items)
    ssm = ssm.reshape(SEQ, HEADS, HEAD_DIM)
    gated = (ssm + head_direct_scale[None, :, None] * xs_f) * jax.nn.silu(output_gate_logits.astype(jnp.float32)).reshape(SEQ, HEADS, HEAD_DIM)
    gated = gated * lax.rsqrt(lax.optimization_barrier(jnp.mean(gated * gated, axis=-1, keepdims=True)) + eps)
    mixed = (gated.reshape(SEQ, INNER) * gated_norm_scale.astype(jnp.float32)).astype(jnp.bfloat16)
    mixer_out = jnp.dot(mixed, mixer_output_weight, preferred_element_type=jnp.float32).astype(jnp.bfloat16)
    tokens_f = second_batch_tokens.astype(jnp.float32)
    normed = (tokens_f * lax.rsqrt(lax.optimization_barrier(jnp.mean(tokens_f * tokens_f, axis=-1, keepdims=True)) + eps) * pre_expert_norm_scale.astype(jnp.float32)).astype(jnp.bfloat16)
    group_logits = jnp.dot(normed, group_router_columns, preferred_element_type=jnp.float32)
    expert_logits = jnp.dot(normed, expert_router_columns, preferred_element_type=jnp.float32)
    weights = route_weights(group_logits, expert_logits, routes)
    block_routes = routes.reshape(N_EP, TOKB, 2)
    positions = jax.vmap(lambda rows: slot_positions(rows, EXPERTS))(block_routes)
    slots = (block_routes.reshape(N_EP, TOKB * 2) * CAP + positions).astype(jnp.int32)
    token_ids = jnp.repeat(jnp.arange(TOKB, dtype=jnp.int32), 2)
    source = jnp.full((N_EP, EXPERTS * CAP), TOKB, jnp.int32)
    source = jax.vmap(lambda row, slot: row.at[slot].set(token_ids))(source, slots)
    padded = jnp.concatenate([normed.reshape(N_EP, TOKB, D), jnp.zeros((N_EP, 1, D), jnp.bfloat16)], axis=1)
    dispatched = jax.vmap(lambda rows, index: jnp.take(rows, index, axis=0))(padded, source)
    per_expert = jnp.transpose(dispatched.reshape(N_EP, EXPERTS, CAP, D), (1, 0, 2, 3)).reshape(EXPERTS, N_EP * CAP, D)
    outputs = lax.map(expert_apply, (per_expert, expert_gate_weight, expert_up_weight, expert_down_weight))
    by_source = jnp.transpose(outputs.reshape(EXPERTS, N_EP, CAP, D), (1, 0, 2, 3)).reshape(N_EP, EXPERTS * CAP, D)
    picked = jax.vmap(lambda rows, index: jnp.take(rows, index, axis=0))(by_source, slots).astype(jnp.float32)
    combined = lax.optimization_barrier(jnp.sum(picked.reshape(N_EP, TOKB, 2, D) * weights.reshape(N_EP, TOKB, 2, 1), axis=2))
    experts_out = combined.reshape(TOKENS, D).astype(jnp.bfloat16)
    return (mixer_out, experts_out)
```

```python
import jax
import jax.numpy as jnp
from jax import lax
from jax.experimental import pallas as pl
from jax.experimental.pallas import tpu as pltpu
from jax.sharding import PartitionSpec as P

HEADS = 32
STATE = 64
GROUPS = 4
BLOCK = 128

eps = 1e-06
exact_prec = lax.Precision.HIGHEST
bf16, f32 = jnp.bfloat16, jnp.float32

NEP = 16
NZ = 8
CAP = 64
HALF = CAP // 2
ORDER = (4, 3, 5, 2, 6, 1, 7, 0)


def kernel(
    tok, nsc, rg, re, rt, gate_h, up_h, down_h, mixed_h, w_h,
    mo, eo,
    nrm, sbuf, xr, gw, uw, dn, hall, ysend, ybuf, zsend, zbuf, wg, mx, psend, precv,
    loc_s, dnl_s, dns_s, dnr_s, xs_s, xr_s, xf_s, xg_s, hs_s, hr_s, ys_s, yr_s, zs_s, zr_s,
    ws_s, wr_s, ms_s, mr_s, fs_s, fr_s,
):
    ep, tp = lax.axis_index("ep"), lax.axis_index("tp")
    y, x = ep // 4, ep % 4
    z, c = tp // 2, tp % 2
    other = z * 2 + (1 - c)

    def ep_at(d, sign):
        return ((y + 4 + sign * (d // 4)) % 4) * 4 + (x + 4 + sign * (d % 4)) % 4

    def tp_at(r):
        return ((z + r) % NZ) * 2 + c

    def push(src, dst, ss, rs, e, t):
        return pltpu.make_async_remote_copy(
            src_ref=src, dst_ref=dst, send_sem=ss, recv_sem=rs,
            device_id={"ep": e, "tp": t}, device_id_type=pl.DeviceIdType.MESH,
        )

    barrier = pltpu.get_barrier_semaphore()

    def greet(e, t):
        pl.semaphore_signal(
            barrier, inc=1, device_id={"ep": e, "tp": t}, device_id_type=pl.DeviceIdType.MESH
        )

    lg = pltpu.make_async_copy(gate_h, gw, loc_s.at[0])
    lu = pltpu.make_async_copy(up_h, uw, loc_s.at[1])
    lw = pltpu.make_async_copy(w_h, wg.at[pl.ds(0, 128), :], loc_s.at[2])
    lm = pltpu.make_async_copy(
        mixed_h.at[pl.ds(pl.multiple_of(z * 256, 256), 256), :], mx.at[:, pl.ds(0, 128)], loc_s.at[3]
    )
    for cp in (lg, lu, lw, lm):
        cp.start()

    def down_cols(q, core):
        return down_h.at[:, pl.ds(pl.multiple_of((2 * ((z + ORDER[q]) % NZ) + core) * 128, 128), 128)]

    dn_l = [
        pltpu.make_async_copy(
            down_cols(q, c), dn.at[c, :, pl.ds(q * 128, 128)], dnl_s.at[q]
        )
        for q in range(NZ)
    ]
    for cp in dn_l:
        cp.start()

    for d in range(1, NEP):
        greet(ep_at(d, 1), tp)
    for r in range(1, NZ):
        greet(ep, tp_at(r))
    greet(ep, other)
    pl.semaphore_wait(barrier, NEP - 1 + NZ - 1 + 1)

    dn_r = [
        push(down_cols(q, 1 - c), dn.at[c, :, pl.ds(q * 128, 128)], dns_s.at[q], dnr_s.at[q], ep, other)
        for q in range(NZ)
    ]
    for cp in dn_r:
        cp.start()
    m_cp = [
        push(
            mixed_h.at[pl.ds(pl.multiple_of(((z + r) % NZ) * 256, 256), 256), :],
            mx.at[:, pl.ds((NZ - r) * 128, 128)],
            ms_s.at[NZ - r], mr_s.at[NZ - r], ep, tp_at(r),
        )
        for r in (4, 3, 5, 2, 6, 1, 7)
    ]
    for cp in m_cp:
        cp.start()

    def w_copy(way, k):
        if way == 0:
            a, b, t = (9 - k) % NZ, NZ - k, tp_at(1)
        else:
            a, b, t = k - 1, k, tp_at(NZ - 1)
        lo, n = (0, 128) if k < 4 else (64 * way, 64)
        src = w_h.at[pl.ds(lo, n), :] if k == 1 else wg.at[pl.ds(a * 128 + lo, n), :]
        return push(
            src, wg.at[pl.ds(b * 128 + lo, n), :], ws_s.at[way, k - 1], wr_s.at[way, k - 1], ep, t
        )

    w_cp = [[w_copy(way, k) for k in range(1, 5)] for way in range(2)]

    def w_step(k):
        for way in range(2):
            if k > 1:
                w_cp[way][k - 2].wait_recv()
            w_cp[way][k - 1].start()

    w_step(1)

    def norm_rows(i, _):
        rows = pl.ds(pl.multiple_of(i * 32, 32), 32)
        v = tok[rows, :].astype(f32)
        v = v * lax.rsqrt(jnp.mean(v * v, axis=1, keepdims=True) + eps) * nsc[...].astype(f32)
        nrm[rows, :] = v.astype(bf16)
        return 0

    lax.fori_loop(0, 8, norm_rows, 0)

    r0, r1 = rt[0:1, :], rt[1:2, :]
    di = lax.broadcasted_iota(jnp.int32, (NEP, 256), 0)
    e_rel = (((y + lax.shift_right_logical(di, 2)) & 3) * 4) + ((x + di) & 3)
    in0, in1 = e_rel == r0, e_rel == r1
    routed = in0 | in1
    onehot = jnp.where(routed, 1.0, 0.0).astype(bf16)
    a = lax.broadcasted_iota(jnp.int32, (256, 256), 0)
    b = lax.broadcasted_iota(jnp.int32, (256, 256), 1)
    before = jnp.where(a < b, 1.0, 0.0).astype(bf16)
    place = jnp.dot(onehot, before, preferred_element_type=f32)
    place = jnp.where(routed, place, -1.0)
    slot = lax.broadcasted_iota(jnp.int32, (HALF, 256), 0) + HALF * c
    slot = slot.astype(f32)
    tokens_n = nrm[...]
    for q in range(4):
        pick = jnp.concatenate(
            [jnp.where(place[d : d + 1, :] == slot, 1.0, 0.0) for d in range(4 * q, 4 * q + 4)], axis=0
        ).astype(bf16)
        sbuf[q * 128 : (q + 1) * 128, :] = jnp.dot(pick, tokens_n, preferred_element_type=f32).astype(bf16)
    x_cp = [
        push(
            sbuf.at[pl.ds(d * HALF, HALF), :],
            xr.at[pl.ds(pl.multiple_of(d * CAP + HALF * c, HALF), HALF), :],
            xs_s.at[d], xr_s.at[d], ep_at(d, 1), tp,
        )
        for d in range(1, NEP)
    ]
    for cp in x_cp:
        cp.start()
    xr[pl.ds(pl.multiple_of(HALF * c, HALF), HALF), :] = sbuf[0:HALF, :]

    nt = (((1,), (1,)), ((), ()))
    gl = lax.dot_general(rg[...], tokens_n, nt, preferred_element_type=f32)
    el = lax.dot_general(re[...], tokens_n, nt, preferred_element_type=f32)

    def lse(v):
        top = jnp.max(v, axis=0, keepdims=True)
        return top + jnp.log(jnp.sum(jnp.exp(v - top), axis=0, keepdims=True))

    gl = gl - lse(gl)
    ei = lax.broadcasted_iota(jnp.int32, (4, 256), 0)
    lp0 = jnp.zeros((1, 256), f32)
    lp1 = jnp.zeros((1, 256), f32)
    for g in range(4):
        part = el[4 * g : 4 * g + 4, :]
        part = part - lse(part) + gl[g : g + 1, :]
        lp0 += jnp.sum(jnp.where(ei + 4 * g == r0, part, 0.0), axis=0, keepdims=True)
        lp1 += jnp.sum(jnp.where(ei + 4 * g == r1, part, 0.0), axis=0, keepdims=True)
    top = jnp.maximum(lp0, lp1)
    w0, w1 = jnp.exp(lp0 - top), jnp.exp(lp1 - top)
    total = w0 + w1
    share = jnp.where(in0, w0 / total, 0.0) + jnp.where(in1, w1 / total, 0.0)
    both = jnp.concatenate([place, share, jnp.zeros((96, 256), f32)], axis=0).T

    lane = lax.broadcasted_iota(jnp.int32, (256, 128), 1)
    in_slot = (lane & (CAP - 1)).astype(f32)
    low = lane < CAP
    mixw = []
    for p in range(8):
        at = jnp.where(low, both[:, 2 * p : 2 * p + 1], both[:, 2 * p + 1 : 2 * p + 2])
        sh = jnp.where(low, both[:, 16 + 2 * p : 17 + 2 * p], both[:, 17 + 2 * p : 18 + 2 * p])
        mixw.append(jnp.where(at == in_slot, sh, 0.0).astype(bf16))
    mixw = jnp.concatenate(mixw, axis=1)

    lg.wait()
    lu.wait()
    for cp in dn_l:
        cp.wait()

    def x_hand(d):
        rows = pl.ds(pl.multiple_of(d * CAP + HALF * c, HALF), HALF)
        return push(xr.at[rows, :], xr.at[rows, :], xf_s.at[d], xg_s.at[d], ep, other)

    hand = [x_hand(d) for d in range(NEP)]

    def y_copy(d, h):
        part = (pl.ds(d * CAP, CAP), pl.ds(h * 512, 512))
        return push(ysend.at[part], ybuf.at[part], ys_s.at[h, d], yr_s.at[h, d], ep_at(d, -1), tp)

    y_cp = [[y_copy(d, h) for d in range(1, NEP)] for h in range(2)]
    h_cp = []
    for g in range(4):
        for d in range(4 * g, 4 * g + 4):
            if d > 0:
                x_cp[d - 1].wait_recv()
            hand[d].start()
        for d in range(4 * g, 4 * g + 4):
            hand[d].wait_recv()
        rows = slice(256 * g, 256 * (g + 1))
        xg = xr[rows, :]
        gv = jnp.dot(xg, gw[...], preferred_element_type=f32)
        uv = jnp.dot(xg, uw[...], preferred_element_type=f32)
        hall[c, rows, :] = (gv * jax.nn.sigmoid(gv) * uv).astype(bf16)
        part = hall.at[c, pl.ds(256 * g, 256), :]
        cp = push(part, part, hs_s.at[g], hr_s.at[g], ep, other)
        cp.start()
        h_cp.append(cp)
        if g == 0:
            for cq in dn_r:
                cq.wait_recv()
        if g == 1:
            w_step(2)
        cp.wait_recv()
        yv = jnp.dot(hall[0, rows, :], dn[0], preferred_element_type=f32)
        yv += jnp.dot(hall[1, rows, :], dn[1], preferred_element_type=f32)
        ysend[rows, :] = yv.astype(bf16)
        for d in range(4 * g, 4 * g + 4):
            if d > 0:
                y_cp[0][d - 1].start()
    for d in range(1, NEP):
        y_cp[1][d - 1].start()
    ybuf[0:CAP, :] = ysend[0:CAP, :]
    w_step(3)

    z_cp = []
    for h in range(2):
        for d in range(1, NEP):
            y_cp[h][d - 1].wait_recv()
        cols = slice(512 * h, 512 * (h + 1))
        comb = jnp.dot(mixw, ybuf[:, cols], preferred_element_type=f32)
        for i in range(4):
            r = ORDER[4 * h + i]
            val = comb[:, 128 * i : 128 * (i + 1)]
            if r == 0:
                zbuf[0] = val.astype(bf16)
                continue
            zsend[r] = val.astype(bf16)
            cp = push(zsend.at[r], zbuf.at[NZ - r], zs_s.at[NZ - r], zr_s.at[NZ - r], ep, tp_at(r))
            cp.start()
            z_cp.append(cp)
        if h == 0:
            w_step(4)

    lw.wait()
    lm.wait()
    for cp in m_cp:
        cp.wait_recv()
    for way in range(2):
        w_cp[way][3].wait_recv()
    theirs = mx[pl.ds(pl.multiple_of((1 - c) * 128, 128), 128), :]
    psend[...] = jnp.dot(theirs, wg[...], preferred_element_type=f32).astype(bf16)
    fin = push(psend, precv, fs_s, fr_s, ep, other)
    fin.start()
    ours = mx[pl.ds(pl.multiple_of(c * 128, 128), 128), :]
    mine = jnp.dot(ours, wg[...], preferred_element_type=f32)
    fin.wait_recv()
    mo[...] = (mine + precv[...].astype(f32)).astype(bf16)

    acc = zbuf[0].astype(f32)
    for cp in z_cp:
        cp.wait_recv()
    for r in range(1, NZ):
        acc += zbuf[r].astype(f32)
    eo[...] = acc.astype(bf16)

    for cp in dn_r + m_cp + x_cp + hand + y_cp[0] + y_cp[1] + h_cp + z_cp + [fin]:
        cp.wait_send()
    for way in range(2):
        for cp in w_cp[way]:
            cp.wait_send()


def fused(tok, nsc, rg, re, rt, gate, up, down, mixed, w):
    vmem, hbm = pl.BlockSpec(memory_space=pltpu.VMEM), pl.BlockSpec(memory_space=pl.ANY)
    dma = pltpu.SemaphoreType.DMA
    v = pltpu.VMEM
    return pl.pallas_call(
        kernel,
        out_shape=(
            jax.ShapeDtypeStruct((128, 2048), bf16),
            jax.ShapeDtypeStruct((256, 128), bf16),
        ),
        in_specs=[vmem] * 5 + [hbm] * 5,
        out_specs=(vmem, vmem),
        scratch_shapes=[
            v((256, 2048), bf16),
            v((512, 2048), bf16),
            v((1024, 2048), bf16),
            v((2048, 256), bf16),
            v((2048, 256), bf16),
            v((2, 256, 1024), bf16),
            v((2, 1024, 256), bf16),
            v((1024, 1024), bf16),
            v((1024, 1024), bf16),
            v((8, 256, 128), bf16),
            v((8, 256, 128), bf16),
            v((1024, 2048), bf16),
            v((256, 1024), bf16),
            v((128, 2048), bf16),
            v((128, 2048), bf16),
            dma((4,)), dma((8,)), dma((8,)), dma((8,)),
            dma((16,)), dma((16,)), dma((16,)), dma((16,)),
            dma((4,)), dma((4,)), dma((2, 16)), dma((2, 16)),
            dma((8,)), dma((8,)), dma((2, 4)), dma((2, 4)), dma((8,)), dma((8,)),
            dma, dma,
        ],
        compiler_params=pltpu.CompilerParams(
            collective_id=0, has_side_effects=True, vmem_limit_bytes=56 * 1024 * 1024
        ),
    )(tok, nsc, rg, re, rt, gate, up, down, mixed, w)


def from_behind(value, axis, steps):
    count = lax.axis_size(axis)
    first, last = (max(0, -steps), min(count, count - steps))
    return lax.ppermute(value, axis, [(source, source + steps) for source in range(first, last)])


def from_everyone(value, axis):
    size = lax.axis_size(axis)
    return lax.all_to_all(
        jnp.broadcast_to(value[None], (size, *value.shape)), axis, 0, 0, tiled=True
    )


def gathered_once(value, axis):
    leaves = jax.tree.leaves(value)
    turns = sorted(range(len(leaves)), key=lambda k: -leaves[k].size)
    width = (1, *leaves[turns[0]].shape)[-1]
    lines = [
        jnp.pad(leaves[k].reshape(-1), (0, -leaves[k].size % width)).reshape(-1, width)
        for k in turns
    ]
    both, at, found = (from_everyone(jnp.concatenate(lines), axis), 0, {})
    for k, line in zip(turns, lines):
        slab = both[:, at : at + len(line)].reshape(len(both), -1)
        found[k] = slab[:, : leaves[k].size].reshape(-1, *leaves[k].shape)
        at += len(line)
    numbers = iter(range(len(leaves)))
    return jax.tree.map(lambda _: found[next(numbers)], value)


def folded_in_pairs(pieces, combine):
    while len(jax.tree.leaves(pieces)[0]) > 1:
        pieces = jax.vmap(combine)(
            *(jax.tree.map(lambda part: part[side::2], pieces) for side in (0, 1))
        )
    return jax.tree.map(lambda part: part[0], pieces)


def entering_2(value, axis, combine, identity):
    size, here = (lax.axis_size(axis), lax.axis_index(axis))
    passed = jnp.arange(size) < here

    def kept(part, zero, own):
        part = jnp.where(
            passed.reshape(-1, *(1 for _ in own.shape)),
            part.astype(own.dtype),
            jnp.asarray(zero, own.dtype),
        )
        return part

    pieces = gathered_once(
        jax.tree.map(lambda part, kind: part.astype(kind), value, (jnp.bfloat16, jnp.bfloat16)),
        axis,
    )
    return folded_in_pairs(jax.tree.map(kept, pieces, identity, value), combine)


def conv_with_rows(joined, before, taps):
    length = joined.shape[0]
    padded = jnp.concatenate([before, joined], axis=0).astype(jnp.float32)
    total = jnp.zeros(joined.shape, jnp.float32)
    for j in range(taps.shape[0]):
        total = total + taps[j].astype(jnp.float32) * padded[j : j + length]
    return jax.nn.silu(total).astype(jnp.bfloat16)


def chain_states(earlier, later):
    return (earlier[0] * later[1][:, None, None] + later[0], earlier[1] * later[1])


def mixer_half(
    mixer_input_channels,
    output_gate_logits,
    head_group_input_map,
    head_group_output_map,
    input_channel_taps,
    input_map_taps,
    output_map_taps,
    step_logits,
    head_log_rate,
    extra_log_decay,
    head_direct_scale,
    gated_norm_scale,
    mixer_output_weight,
):
    length, width = mixer_input_channels.shape
    heads_dev = head_direct_scale.shape[0]
    head_dim = width // heads_dev
    group = lax.axis_index("tp") * heads_dev // (HEADS // GROUPS)
    first_col = group * STATE
    b_rows = lax.dynamic_slice_in_dim(head_group_input_map, first_col, STATE, 1)
    c_rows = lax.dynamic_slice_in_dim(head_group_output_map, first_col, STATE, 1)
    b_taps = lax.dynamic_slice_in_dim(input_map_taps, first_col, STATE, 1)
    c_taps = lax.dynamic_slice_in_dim(output_map_taps, first_col, STATE, 1)
    joined = jnp.concatenate([mixer_input_channels, b_rows, c_rows], axis=1)
    taps = jnp.concatenate([input_channel_taps, b_taps, c_taps], axis=1)
    reach = taps.shape[0] - 1
    before = from_behind(joined[length - reach :], "ep", 1)
    conv = conv_with_rows(joined, before, taps)
    nblk = length // BLOCK
    xs_f = conv[:, :width].astype(jnp.float32)
    bs_f = conv[:, width : width + STATE].astype(jnp.float32).reshape(nblk, BLOCK, STATE)
    cs_f = conv[:, width + STATE :].astype(jnp.float32).reshape(nblk, BLOCK, STATE)
    head_step_length = jax.nn.softplus(step_logits)
    position_log_decay = extra_log_decay - head_step_length * jnp.exp(head_log_rate)[:, None]
    cum = jnp.cumsum(position_log_decay.reshape(heads_dev, nblk, BLOCK), axis=2)
    step_blocks = jnp.transpose(head_step_length.reshape(heads_dev, nblk, BLOCK), (1, 2, 0))
    x_dt = xs_f.reshape(nblk, BLOCK, heads_dev, head_dim) * step_blocks[..., None]
    lower = jnp.tril(jnp.ones((BLOCK, BLOCK), bool))
    diff = cum[:, :, :, None] - cum[:, :, None, :]
    weight = jnp.where(lower, jnp.exp(jnp.where(lower, diff, 0.0)), 0.0)
    scores = jnp.einsum("bln,bsn->bls", cs_f, bs_f, precision=exact_prec)
    inner = jnp.einsum("bls,hbls,bshp->blhp", scores, weight, x_dt, precision=exact_prec)
    tail = jnp.exp(cum[:, :, -1:] - cum)
    block_state = jnp.einsum("bsn,hbs,bshp->bhpn", bs_f, tail, x_dt, precision=exact_prec)
    block_log = cum[:, :, -1]
    run_log = jnp.cumsum(block_log, axis=1)
    total_log = run_log[:, -1]
    own_state = jnp.einsum(
        "hb,bhpn->hpn", jnp.exp(total_log[:, None] - run_log), block_state, precision=exact_prec
    )
    own_decay = jnp.exp(total_log)
    entering, reached = entering_2(
        (own_state, own_decay),
        "ep",
        chain_states,
        (jnp.zeros_like(own_state), jnp.ones_like(own_decay)),
    )
    start_log = run_log - block_log
    earlier = jnp.arange(nblk)[:, None] > jnp.arange(nblk)[None, :]
    gap = start_log[:, :, None] - run_log[:, None, :]
    link = jnp.where(earlier, jnp.exp(jnp.where(earlier, gap, 0.0)), 0.0)
    prev = jnp.einsum("hbc,chpn->bhpn", link, block_state, precision=exact_prec)
    prev = prev + jnp.transpose(jnp.exp(start_log))[:, :, None, None] * entering[None]
    carried = jnp.einsum("bln,bhpn->blhp", cs_f, prev, precision=exact_prec)
    carried = carried * jnp.transpose(jnp.exp(cum), (1, 2, 0))[..., None]
    ssm = (inner + carried).reshape(length, heads_dev, head_dim)
    gated = (
        ssm + head_direct_scale[None, :, None] * xs_f.reshape(length, heads_dev, head_dim)
    ) * jax.nn.silu(output_gate_logits.astype(jnp.float32)).reshape(length, heads_dev, head_dim)
    gated = gated * lax.rsqrt(jnp.mean(gated * gated, axis=-1, keepdims=True) + eps)
    mixed = (gated.reshape(length, width) * gated_norm_scale.astype(jnp.float32)).astype(
        jnp.bfloat16
    )
    return mixed


def per_device(
    mixer_input_channels,
    output_gate_logits,
    head_group_input_map,
    head_group_output_map,
    input_channel_taps,
    input_map_taps,
    output_map_taps,
    step_logits,
    head_log_rate,
    extra_log_decay,
    head_direct_scale,
    gated_norm_scale,
    mixer_output_weight,
    second_batch_tokens,
    pre_expert_norm_scale,
    group_router_columns,
    expert_router_columns,
    routes,
    expert_gate_weight,
    expert_up_weight,
    expert_down_weight,
):
    mixed = mixer_half(
        mixer_input_channels,
        output_gate_logits,
        head_group_input_map,
        head_group_output_map,
        input_channel_taps,
        input_map_taps,
        output_map_taps,
        step_logits,
        head_log_rate,
        extra_log_decay,
        head_direct_scale,
        gated_norm_scale,
        mixer_output_weight,
    )
    return fused(
        second_batch_tokens,
        pre_expert_norm_scale.reshape(1, -1),
        group_router_columns.T,
        expert_router_columns.T,
        routes.T,
        expert_gate_weight[0],
        expert_up_weight[0],
        expert_down_weight[0],
        mixed,
        mixer_output_weight,
    )


def solution(mesh):
    in_specs = (
        P("ep", "tp"),
        P("ep", "tp"),
        P("ep", None),
        P("ep", None),
        P(None, "tp"),
        P(),
        P(),
        P("tp", "ep"),
        P("tp"),
        P("tp", "ep"),
        P("tp"),
        P("tp"),
        P("tp", None),
        P("ep", None),
        P(),
        P(),
        P(),
        P("ep", None),
        P("ep", None, "tp"),
        P("ep", None, "tp"),
        P("ep", "tp", None),
    )
    out_specs = (P(("ep", "tp"), None), P("ep", "tp"))
    return jax.shard_map(
        per_device, mesh=mesh, in_specs=in_specs, out_specs=out_specs, check_vma=False
    )
```

```python
import jax
import jax.numpy as jnp
from jax import lax
from jax.experimental import pallas as pl
from jax.experimental.pallas import tpu as pltpu
from jax.sharding import PartitionSpec as P

eps = 1e-06
exact_prec = lax.Precision.HIGHEST
bf16, f32 = jnp.bfloat16, jnp.float32

NEP = 16
NZ = 8
CAP = 64
HALF = CAP // 2
ORDER = (4, 3, 5, 2, 6, 1, 7, 0)


def kernel(
    tok, nsc, rg, re, rt, ut, bt, ct, sl, ex, gn, rate, direct,
    gate_h, up_h, down_h, w_h, u_h, og_h, bm_h, cm_h,
    mo, eo,
    nrm, sbuf, xr, gw, uw, dn, hall, ysend, ybuf, zsend, zbuf, wg, mx, psend, precv,
    ub, bb, cb, ogb, xsb, csb, c0l, c1l, dtl, cumr, dtr, tst, ssm, spad, ssend, sst, entb, mixb,
    loc_s, dnl_s, dns_s, dnr_s, xs_s, xr_s, xf_s, xg_s, hs_s, hr_s, ys_s, yr_s, zs_s, zr_s,
    ws_s, wr_s, ms_s, mr_s, fs_s, fr_s, hl_s, hh_s, ss_s, sr_s,
):
    ep, tp = lax.axis_index("ep"), lax.axis_index("tp")
    y, x = ep // 4, ep % 4
    z, c = tp // 2, tp % 2
    other = z * 2 + (1 - c)

    def ep_at(d, sign):
        return ((y + 4 + sign * (d // 4)) % 4) * 4 + (x + 4 + sign * (d % 4)) % 4

    def tp_at(r):
        return ((z + r) % NZ) * 2 + c

    def push(src, dst, ss, rs, e, t):
        return pltpu.make_async_remote_copy(
            src_ref=src, dst_ref=dst, send_sem=ss, recv_sem=rs,
            device_id={"ep": e, "tp": t}, device_id_type=pl.DeviceIdType.MESH,
        )

    barrier = pltpu.get_barrier_semaphore()

    def greet(e, t):
        pl.semaphore_signal(
            barrier, inc=1, device_id={"ep": e, "tp": t}, device_id_type=pl.DeviceIdType.MESH
        )

    lg = pltpu.make_async_copy(gate_h, gw, loc_s.at[0])
    lu = pltpu.make_async_copy(up_h, uw, loc_s.at[1])
    lw = pltpu.make_async_copy(w_h, wg.at[pl.ds(0, 128), :], loc_s.at[2])
    grp = tp // 4
    map_cols = pl.ds(pl.multiple_of((grp // 2) * 128, 128), 128)
    body, tail = pl.ds(8, 2048), pl.ds(2040, 8)
    l_mix = [
        pltpu.make_async_copy(u_h, ub.at[body, :], loc_s.at[4]),
        pltpu.make_async_copy(bm_h.at[:, map_cols], bb.at[body, :], loc_s.at[5]),
        pltpu.make_async_copy(cm_h.at[:, map_cols], cb.at[body, :], loc_s.at[6]),
        pltpu.make_async_copy(og_h, ogb, loc_s.at[3]),
    ]
    for cp in l_mix + [lg, lu, lw]:
        cp.start()

    def down_cols(q, core):
        return down_h.at[:, pl.ds(pl.multiple_of((2 * ((z + ORDER[q]) % NZ) + core) * 128, 128), 128)]

    dn_l = [
        pltpu.make_async_copy(
            down_cols(q, c), dn.at[c, :, pl.ds(q * 128, 128)], dnl_s.at[q]
        )
        for q in range(NZ)
    ]
    for cp in dn_l:
        cp.start()

    for d in range(1, NEP):
        greet(ep_at(d, 1), tp)
    for r in range(1, NZ):
        greet(ep, tp_at(r))
    greet(ep, other)
    def norm_rows(i, _):
        rows = pl.ds(pl.multiple_of(i * 32, 32), 32)
        v = tok[rows, :].astype(f32)
        v = v * lax.rsqrt(jnp.mean(v * v, axis=1, keepdims=True) + eps) * nsc[...].astype(f32)
        nrm[rows, :] = v.astype(bf16)
        return 0

    lax.fori_loop(0, 8, norm_rows, 0)

    r0, r1 = rt[0:1, :], rt[1:2, :]
    di = lax.broadcasted_iota(jnp.int32, (NEP, 256), 0)
    e_rel = (((y + lax.shift_right_logical(di, 2)) & 3) * 4) + ((x + di) & 3)
    in0, in1 = e_rel == r0, e_rel == r1
    routed = in0 | in1
    onehot = jnp.where(routed, 1.0, 0.0).astype(bf16)
    a = lax.broadcasted_iota(jnp.int32, (256, 256), 0)
    b = lax.broadcasted_iota(jnp.int32, (256, 256), 1)
    before = jnp.where(a < b, 1.0, 0.0).astype(bf16)
    place = jnp.dot(onehot, before, preferred_element_type=f32)
    place = jnp.where(routed, place, -1.0)
    slot = lax.broadcasted_iota(jnp.int32, (HALF, 256), 0) + HALF * c
    slot = slot.astype(f32)
    tokens_n = nrm[...]
    for q in range(4):
        pick = jnp.concatenate(
            [jnp.where(place[d : d + 1, :] == slot, 1.0, 0.0) for d in range(4 * q, 4 * q + 4)], axis=0
        ).astype(bf16)
        sbuf[q * 128 : (q + 1) * 128, :] = jnp.dot(pick, tokens_n, preferred_element_type=f32).astype(bf16)
    pl.semaphore_wait(barrier, NEP - 1 + NZ - 1 + 1)
    after = (ep + 1) % NEP
    halo = [
        push(u_h.at[tail, :], ub.at[pl.ds(0, 8), :], hl_s.at[0], hh_s.at[0], after, tp),
        push(bm_h.at[tail, map_cols], bb.at[pl.ds(0, 8), :], hl_s.at[1], hh_s.at[1], after, tp),
        push(cm_h.at[tail, map_cols], cb.at[pl.ds(0, 8), :], hl_s.at[2], hh_s.at[2], after, tp),
    ]
    for cp in halo:
        cp.start()

    dn_r = [
        push(down_cols(q, 1 - c), dn.at[c, :, pl.ds(q * 128, 128)], dns_s.at[q], dnr_s.at[q], ep, other)
        for q in range(NZ)
    ]
    for cp in dn_r:
        cp.start()
    def w_copy(way, k):
        if way == 0:
            a, b, t = (9 - k) % NZ, NZ - k, tp_at(1)
        else:
            a, b, t = k - 1, k, tp_at(NZ - 1)
        lo, n = (0, 128) if k < 4 else (64 * way, 64)
        src = w_h.at[pl.ds(lo, n), :] if k == 1 else wg.at[pl.ds(a * 128 + lo, n), :]
        return push(
            src, wg.at[pl.ds(b * 128 + lo, n), :], ws_s.at[way, k - 1], wr_s.at[way, k - 1], ep, t
        )

    w_cp = [[w_copy(way, k) for k in range(1, 5)] for way in range(2)]

    def w_step(k):
        for way in range(2):
            if k > 1:
                w_cp[way][k - 2].wait_recv()
            w_cp[way][k - 1].start()

    w_step(1)

    x_cp = [
        push(
            sbuf.at[pl.ds(d * HALF, HALF), :],
            xr.at[pl.ds(pl.multiple_of(d * CAP + HALF * c, HALF), HALF), :],
            xs_s.at[d], xr_s.at[d], ep_at(d, 1), tp,
        )
        for d in range(1, NEP)
    ]
    for cp in x_cp[:7]:
        cp.start()
    xr[pl.ds(pl.multiple_of(HALF * c, HALF), HALF), :] = sbuf[0:HALF, :]

    nt = (((1,), (1,)), ((), ()))
    gl = lax.dot_general(rg[...], tokens_n, nt, preferred_element_type=f32)
    el = lax.dot_general(re[...], tokens_n, nt, preferred_element_type=f32)

    def lse(v):
        top = jnp.max(v, axis=0, keepdims=True)
        return top + jnp.log(jnp.sum(jnp.exp(v - top), axis=0, keepdims=True))

    gl = gl - lse(gl)
    ei = lax.broadcasted_iota(jnp.int32, (4, 256), 0)
    lp0 = jnp.zeros((1, 256), f32)
    lp1 = jnp.zeros((1, 256), f32)
    for g in range(4):
        part = el[4 * g : 4 * g + 4, :]
        part = part - lse(part) + gl[g : g + 1, :]
        lp0 += jnp.sum(jnp.where(ei + 4 * g == r0, part, 0.0), axis=0, keepdims=True)
        lp1 += jnp.sum(jnp.where(ei + 4 * g == r1, part, 0.0), axis=0, keepdims=True)
    top = jnp.maximum(lp0, lp1)
    w0, w1 = jnp.exp(lp0 - top), jnp.exp(lp1 - top)
    total = w0 + w1
    share = jnp.where(in0, w0 / total, 0.0) + jnp.where(in1, w1 / total, 0.0)
    both = jnp.concatenate([place, share, jnp.zeros((96, 256), f32)], axis=0).T

    lane = lax.broadcasted_iota(jnp.int32, (256, 128), 1)
    in_slot = (lane & (CAP - 1)).astype(f32)
    low = lane < CAP
    mixw = []
    for p in range(8):
        at = jnp.where(low, both[:, 2 * p : 2 * p + 1], both[:, 2 * p + 1 : 2 * p + 2])
        sh = jnp.where(low, both[:, 16 + 2 * p : 17 + 2 * p], both[:, 17 + 2 * p : 18 + 2 * p])
        mixw.append(jnp.where(at == in_slot, sh, 0.0).astype(bf16))
    mixw = jnp.concatenate(mixw, axis=1)

    row = lax.broadcasted_iota(jnp.int32, (32, 128), 0)
    lane1 = lax.broadcasted_iota(jnp.int32, (1, 128), 1)
    first = lax.broadcasted_iota(jnp.int32, (128, 128), 1) < 64
    at_l = lax.broadcasted_iota(jnp.int32, (128, 128), 0)
    at_s = lax.broadcasted_iota(jnp.int32, (128, 128), 1)
    lower = at_l >= at_s
    sv = sl[...]
    dt = jnp.maximum(sv, 0.0) + jnp.log1p(jnp.exp(-jnp.abs(sv)))
    speed = jnp.exp(jnp.where((row & 1) == 0, rate[0], rate[1]))
    log_decay = ex[...] - dt * speed
    upto = jnp.where(at_l <= at_s, 1.0, 0.0).astype(f32)
    cum = jnp.dot(log_decay, upto, precision=exact_prec, preferred_element_type=f32)
    cumr[...] = cum
    dtr[...] = dt
    turned = jnp.concatenate([cum, dt, jnp.zeros((64, 128), f32)], axis=0).T
    for b in range(16):
        rows = slice(128 * b, 128 * (b + 1))
        c0l[rows, :] = jnp.broadcast_to(turned[:, 2 * b : 2 * b + 1], (128, 128))
        c1l[rows, :] = jnp.broadcast_to(turned[:, 2 * b + 1 : 2 * b + 2], (128, 128))
        dtl[rows, :] = jnp.where(first, turned[:, 32 + 2 * b : 33 + 2 * b], turned[:, 33 + 2 * b : 34 + 2 * b])

    for cp in l_mix:
        cp.wait()
    for cp in halo:
        cp.wait_recv()
    for buf in (ub, bb, cb):
        edge = buf[0:8, :]
        buf[0:8, :] = jnp.where(ep == 0, jnp.zeros_like(edge), edge)
    tap_u = ut[...].astype(f32)
    block_0 = grp // 2 == 0
    tap_b = jnp.where(block_0, bt[:, 0:128].astype(f32), bt[:, 128:256].astype(f32))
    tap_c = jnp.where(block_0, ct[:, 0:128].astype(f32), ct[:, 128:256].astype(f32))
    own_half = (lane1 // 64) == grp % 2

    def conv(buf, taps, base):
        ext = buf[pl.ds(base, 136), :].astype(f32)
        tot = taps[0:1, :] * ext[5:133, :]
        for j in range(1, 4):
            tot += taps[j : j + 1, :] * ext[5 + j : 133 + j, :]
        return tot * jax.nn.sigmoid(tot)

    def one_block(b, carry):
        state, since = carry
        base = pl.multiple_of(b * 128, 128)
        rows = pl.ds(base, 128)
        xs = conv(ub, tap_u, base).astype(bf16)
        bs = conv(bb, tap_b, base).astype(bf16)
        cs = jnp.where(own_half, conv(cb, tap_c, base), 0.0).astype(bf16)
        xsb[rows, :] = xs
        csb[rows, :] = cs
        tst[pl.ds(b, 1), :] = since
        scores = lax.dot_general(cs, bs, (((1,), (1,)), ((), ())), preferred_element_type=f32)
        inner = []
        for h, col in ((0, c0l), (1, c1l)):
            at = pl.ds(2 * b + h, 1)
            diff = jnp.where(lower, col[rows, :] - cumr[at, :], 0.0)
            near = jnp.where(lower, scores * jnp.exp(diff) * dtr[at, :], 0.0).astype(bf16)
            inner.append(jnp.dot(near, xs, preferred_element_type=f32))
        both_cum = jnp.where(first, c0l[rows, :], c1l[rows, :])
        carried = jnp.dot(cs, state.astype(bf16), preferred_element_type=f32) * jnp.exp(both_cum)
        ssm[rows, :] = jnp.where(first, inner[0], inner[1]) + carried
        last = both_cum[127:128, :]
        weighed = (xs.astype(f32) * (jnp.exp(last - both_cum) * dtl[rows, :])).astype(bf16)
        gained = lax.dot_general(bs, weighed, (((0,), (0,)), ((), ())), preferred_element_type=f32)
        return state * jnp.exp(last) + gained, since + last

    state, since = lax.fori_loop(
        0, 16, one_block, (jnp.zeros((128, 128), f32), jnp.zeros((1, 128), f32))
    )
    spad[...] = state
    half_rows = pl.ds(pl.multiple_of((grp % 2) * 64, 64), 64)
    ssend[0:64, :] = spad[half_rows, :].astype(bf16)
    decay = jnp.exp(since)
    near_decay = decay.astype(bf16)
    rest_decay = (decay - near_decay.astype(f32)).astype(bf16)
    row8 = lax.broadcasted_iota(jnp.int32, (8, 128), 0)
    ssend[64:72, :] = jnp.where(
        row8 == 0, near_decay.astype(f32), jnp.where(row8 == 1, rest_decay.astype(f32), 0.0)
    ).astype(bf16)
    s_cp = [
        push(ssend, sst.at[ep], ss_s.at[d], sr_s.at[d], ep_at(d, 1), tp) for d in range(1, NEP)
    ]
    for cp in s_cp:
        cp.start()
    for cp in x_cp[7:]:
        cp.start()
    w_step(2)


    def mixer_rest():
        for cp in s_cp:
            cp.wait_recv()

        def chain(j, ent):
            got = sst[j].astype(f32)
            return jnp.where(j < ep, ent * (got[64:65, :] + got[65:66, :]) + got[0:64, :], ent)

        ent = lax.fori_loop(0, NEP - 1, chain, jnp.zeros((64, 128), f32))
        entb[...] = jnp.zeros_like(entb)
        entb[half_rows, :] = ent.astype(bf16)
        scale = jnp.where(lane1 < 64, direct[0], direct[1])
        gain = gn[...].astype(f32)

        def rows_of(j, keep):
            for k in range(2):
                b = 2 * j + k
                rows = pl.ds(pl.multiple_of(b * 128, 128), 128)
                since_b = jnp.where(first, c0l[rows, :], c1l[rows, :]) + tst[pl.ds(b, 1), :]
                far = jnp.dot(csb[rows, :], entb[...], preferred_element_type=f32) * jnp.exp(since_b)
                gate = ogb[rows, :].astype(f32)
                val = (ssm[rows, :] + far + scale * xsb[rows, :].astype(f32)) * (gate * jax.nn.sigmoid(gate))
                sq = val * val
                sum0 = jnp.sum(jnp.where(first, sq, 0.0), axis=1, keepdims=True)
                sum1 = jnp.sum(jnp.where(first, 0.0, sq), axis=1, keepdims=True)
                ms = jnp.where(first, sum0, sum1) * (1.0 / 64)
                keep(k, rows, (val * lax.rsqrt(ms + eps) * gain).astype(bf16))

        def send_on(i, _):
            j = (z + 1 + i) % NZ

            def keep(k, rows, val):
                mixb[rows, :] = val

            rows_of(j, keep)
            push(
                mixb.at[pl.ds(pl.multiple_of(j * 256, 256), 256), :],
                mx.at[:, pl.ds(pl.multiple_of((7 - i) * 128, 128), 128)],
                ms_s.at[7 - i], mr_s.at[7 - i], ep, tp_at(1 + i),
            ).start()
            return 0

        lax.fori_loop(0, NZ - 1, send_on, 0)

        def own(k, rows, val):
            mx[128 * k : 128 * (k + 1), 0:128] = val

        rows_of(z, own)

    m_cp = [
        push(
            mixb.at[pl.ds(pl.multiple_of(((z + r) % NZ) * 256, 256), 256), :],
            mx.at[:, pl.ds((NZ - r) * 128, 128)],
            ms_s.at[NZ - r], mr_s.at[NZ - r], ep, tp_at(r),
        )
        for r in range(1, NZ)
    ]

    lg.wait()
    lu.wait()
    for cp in dn_l:
        cp.wait()

    def x_hand(d):
        rows = pl.ds(pl.multiple_of(d * CAP + HALF * c, HALF), HALF)
        return push(xr.at[rows, :], xr.at[rows, :], xf_s.at[d], xg_s.at[d], ep, other)

    hand = [x_hand(d) for d in range(NEP)]

    def y_copy(d, h):
        part = (pl.ds(d * CAP, CAP), pl.ds(h * 512, 512))
        return push(ysend.at[part], ybuf.at[part], ys_s.at[h, d], yr_s.at[h, d], ep_at(d, -1), tp)

    y_cp = [[y_copy(d, h) for d in range(1, NEP)] for h in range(2)]
    h_cp = []
    for g in range(4):
        for d in range(4 * g, 4 * g + 4):
            if d > 0:
                x_cp[d - 1].wait_recv()
            hand[d].start()
        for d in range(4 * g, 4 * g + 4):
            hand[d].wait_recv()
        rows = slice(256 * g, 256 * (g + 1))
        xg = xr[rows, :]
        gv = jnp.dot(xg, gw[...], preferred_element_type=f32)
        uv = jnp.dot(xg, uw[...], preferred_element_type=f32)
        hall[c, rows, :] = (gv * jax.nn.sigmoid(gv) * uv).astype(bf16)
        part = hall.at[c, pl.ds(256 * g, 256), :]
        cp = push(part, part, hs_s.at[g], hr_s.at[g], ep, other)
        cp.start()
        h_cp.append(cp)
        if g == 0:
            for cq in dn_r:
                cq.wait_recv()
        if g == 2:
            w_step(3)
            mixer_rest()
        cp.wait_recv()
        yv = jnp.dot(hall[0, rows, :], dn[0], preferred_element_type=f32)
        yv += jnp.dot(hall[1, rows, :], dn[1], preferred_element_type=f32)
        ysend[rows, :] = yv.astype(bf16)
        for d in range(4 * g, 4 * g + 4):
            if d > 0:
                y_cp[0][d - 1].start()
    for d in range(1, NEP):
        y_cp[1][d - 1].start()
    ybuf[0:CAP, :] = ysend[0:CAP, :]

    z_cp = []
    for h in range(2):
        for d in range(1, NEP):
            y_cp[h][d - 1].wait_recv()
        cols = slice(512 * h, 512 * (h + 1))
        comb = jnp.dot(mixw, ybuf[:, cols], preferred_element_type=f32)
        for i in range(4):
            r = ORDER[4 * h + i]
            val = comb[:, 128 * i : 128 * (i + 1)]
            if r == 0:
                zbuf[0] = val.astype(bf16)
                continue
            zsend[r] = val.astype(bf16)
            cp = push(zsend.at[r], zbuf.at[NZ - r], zs_s.at[NZ - r], zr_s.at[NZ - r], ep, tp_at(r))
            cp.start()
            z_cp.append(cp)
        if h == 0:
            w_step(4)

    lw.wait()
    for cp in m_cp:
        cp.wait_recv()
    for way in range(2):
        w_cp[way][3].wait_recv()
    theirs = mx[pl.ds(pl.multiple_of((1 - c) * 128, 128), 128), :]
    psend[...] = jnp.dot(theirs, wg[...], preferred_element_type=f32).astype(bf16)
    fin = push(psend, precv, fs_s, fr_s, ep, other)
    fin.start()
    ours = mx[pl.ds(pl.multiple_of(c * 128, 128), 128), :]
    mine = jnp.dot(ours, wg[...], preferred_element_type=f32)
    fin.wait_recv()
    mo[...] = (mine + precv[...].astype(f32)).astype(bf16)

    acc = zbuf[0].astype(f32)
    for cp in z_cp:
        cp.wait_recv()
    for r in range(1, NZ):
        acc += zbuf[r].astype(f32)
    eo[...] = acc.astype(bf16)

    for cp in dn_r + m_cp + x_cp + halo + s_cp + hand + y_cp[0] + y_cp[1] + h_cp + z_cp + [fin]:
        cp.wait_send()
    for way in range(2):
        for cp in w_cp[way]:
            cp.wait_send()


def fused(*args):
    vmem, hbm = pl.BlockSpec(memory_space=pltpu.VMEM), pl.BlockSpec(memory_space=pl.ANY)
    smem = pl.BlockSpec(memory_space=pltpu.SMEM)
    dma = pltpu.SemaphoreType.DMA
    v = pltpu.VMEM
    return pl.pallas_call(
        kernel,
        out_shape=(
            jax.ShapeDtypeStruct((128, 2048), bf16),
            jax.ShapeDtypeStruct((256, 128), bf16),
        ),
        in_specs=[vmem] * 11 + [smem] * 2 + [hbm] * 8,
        out_specs=(vmem, vmem),
        scratch_shapes=[
            v((256, 2048), bf16),
            v((512, 2048), bf16),
            v((1024, 2048), bf16),
            v((2048, 256), bf16),
            v((2048, 256), bf16),
            v((2, 256, 1024), bf16),
            v((2, 1024, 256), bf16),
            v((1024, 1024), bf16),
            v((1024, 1024), bf16),
            v((8, 256, 128), bf16),
            v((8, 256, 128), bf16),
            v((1024, 2048), bf16),
            v((256, 1024), bf16),
            v((128, 2048), bf16),
            v((128, 2048), bf16),
            v((2056, 128), bf16),
            v((2056, 128), bf16),
            v((2056, 128), bf16),
            v((2048, 128), bf16),
            v((2048, 128), bf16),
            v((2048, 128), bf16),
            v((2048, 128), f32),
            v((2048, 128), f32),
            v((2048, 128), f32),
            v((32, 128), f32),
            v((32, 128), f32),
            v((16, 128), f32),
            v((2048, 128), f32),
            v((128, 128), f32),
            v((72, 128), bf16),
            v((16, 72, 128), bf16),
            v((128, 128), bf16),
            v((2048, 128), bf16),
            dma((7,)), dma((8,)), dma((8,)), dma((8,)),
            dma((16,)), dma((16,)), dma((16,)), dma((16,)),
            dma((4,)), dma((4,)), dma((2, 16)), dma((2, 16)),
            dma((8,)), dma((8,)), dma((2, 4)), dma((2, 4)), dma((8,)), dma((8,)),
            dma, dma, dma((3,)), dma((3,)), dma((16,)), dma((16,)),
        ],
        compiler_params=pltpu.CompilerParams(
            collective_id=0, has_side_effects=True, vmem_limit_bytes=56 * 1024 * 1024
        ),
    )(*args)


def per_device(
    mixer_input_channels,
    output_gate_logits,
    head_group_input_map,
    head_group_output_map,
    input_channel_taps,
    input_map_taps,
    output_map_taps,
    step_logits,
    head_log_rate,
    extra_log_decay,
    head_direct_scale,
    gated_norm_scale,
    mixer_output_weight,
    second_batch_tokens,
    pre_expert_norm_scale,
    group_router_columns,
    expert_router_columns,
    routes,
    expert_gate_weight,
    expert_up_weight,
    expert_down_weight,
):
    def by_block(v):
        return jnp.transpose(v.reshape(2, 16, 128), (1, 0, 2)).reshape(32, 128)

    return fused(
        second_batch_tokens,
        pre_expert_norm_scale.reshape(1, -1),
        group_router_columns.T,
        expert_router_columns.T,
        routes.T,
        input_channel_taps,
        input_map_taps,
        output_map_taps,
        by_block(step_logits),
        by_block(extra_log_decay),
        gated_norm_scale.reshape(1, -1),
        head_log_rate,
        head_direct_scale,
        expert_gate_weight[0],
        expert_up_weight[0],
        expert_down_weight[0],
        mixer_output_weight,
        mixer_input_channels,
        output_gate_logits,
        head_group_input_map,
        head_group_output_map,
    )


def solution(mesh):
    in_specs = (
        P("ep", "tp"),
        P("ep", "tp"),
        P("ep", None),
        P("ep", None),
        P(None, "tp"),
        P(),
        P(),
        P("tp", "ep"),
        P("tp"),
        P("tp", "ep"),
        P("tp"),
        P("tp"),
        P("tp", None),
        P("ep", None),
        P(),
        P(),
        P(),
        P("ep", None),
        P("ep", None, "tp"),
        P("ep", None, "tp"),
        P("ep", "tp", None),
    )
    out_specs = (P(("ep", "tp"), None), P("ep", "tp"))
    return jax.shard_map(
        per_device, mesh=mesh, in_specs=in_specs, out_specs=out_specs, check_vma=False
    )
```

```python
import jax
import jax.numpy as jnp
from jax import lax
from jax.experimental import pallas as pl
from jax.experimental.pallas import tpu as pltpu
from jax.sharding import PartitionSpec as P

eps = 1e-06
exact_prec = lax.Precision.HIGHEST
bf16, f32 = jnp.bfloat16, jnp.float32

NEP = 16
NZ = 8
CAP = 64
HALF = CAP // 2
ORDER = (4, 3, 5, 2, 6, 1, 7, 0)
NEAR = (
    (0, 0), (1, 0), (0, 1), (3, 0), (0, 3), (1, 1), (3, 3), (1, 3),
    (3, 1), (2, 0), (0, 2), (2, 1), (1, 2), (3, 2), (2, 3), (2, 2),
)
EARLY = 12


def kernel(
    nsc, rg, re, rt, ut, bt, ct, sl, ex, gn, rate, direct,
    tok_h, gate_h, up_h, down_h, w_h, u_h, og_h, bm_h, cm_h,
    mo, eo,
    nrm, sbuf, xr, gw, uw, dn, hall, ysend, ybuf, zsend, zbuf, wg, mx, psend, precv,
    ub, bb, cb, ogb, xsb, csb, c0l, c1l, dtl, cumr, dtr, tst, ssm, spad, ssend, sst, entb, mixb, keep_mine, tok,
    loc_s, dnl_s, dns_s, dnr_s, xs_s, xr_s, xf_s, xg_s, hs_s, hr_s, ys_s, yr_s, zs_s, zr_s,
    ws_s, wr_s, ms_s, mr_s, fs_s, fr_s, hl_s, hh_s, ss_s, sr_s,
):
    ep, tp = lax.axis_index("ep"), lax.axis_index("tp")
    y, x = ep // 4, ep % 4
    z, c = tp // 2, tp % 2
    other = z * 2 + (1 - c)

    def ep_at(d, sign):
        dx, dy = NEAR[d]
        return ((y + 4 + sign * dy) % 4) * 4 + (x + 4 + sign * dx) % 4

    def tp_at(r):
        return ((z + r) % NZ) * 2 + c

    def push(src, dst, ss, rs, e, t):
        return pltpu.make_async_remote_copy(
            src_ref=src, dst_ref=dst, send_sem=ss, recv_sem=rs,
            device_id={"ep": e, "tp": t}, device_id_type=pl.DeviceIdType.MESH,
        )

    barrier = pltpu.get_barrier_semaphore()

    def greet(e, t):
        pl.semaphore_signal(
            barrier, inc=1, device_id={"ep": e, "tp": t}, device_id_type=pl.DeviceIdType.MESH
        )

    for d in range(1, NEP):
        greet(ep_at(d, 1), tp)
    for r in range(1, NZ):
        greet(ep, tp_at(r))
    greet(ep, other)

    lt = pltpu.make_async_copy(tok_h, tok, loc_s.at[7])
    lt.start()
    lg = pltpu.make_async_copy(gate_h, gw, loc_s.at[0])
    lu = pltpu.make_async_copy(up_h, uw, loc_s.at[1])
    lw = pltpu.make_async_copy(w_h, wg.at[pl.ds(0, 128), :], loc_s.at[2])
    grp = tp // 4
    map_cols = pl.ds(pl.multiple_of((grp // 2) * 128, 128), 128)
    body, tail = pl.ds(8, 2048), pl.ds(2040, 8)
    l_mix = [
        pltpu.make_async_copy(u_h, ub.at[body, :], loc_s.at[4]),
        pltpu.make_async_copy(bm_h.at[:, map_cols], bb.at[body, :], loc_s.at[5]),
        pltpu.make_async_copy(cm_h.at[:, map_cols], cb.at[body, :], loc_s.at[6]),
        pltpu.make_async_copy(og_h, ogb, loc_s.at[3]),
    ]
    for cp in l_mix + [lg, lu, lw]:
        cp.start()

    def down_cols(q, core):
        return down_h.at[:, pl.ds(pl.multiple_of((2 * ((z + ORDER[q]) % NZ) + core) * 128, 128), 128)]

    dn_l = [
        pltpu.make_async_copy(
            down_cols(q, c), dn.at[c, :, pl.ds(q * 128, 128)], dnl_s.at[q]
        )
        for q in range(NZ)
    ]
    for cp in dn_l:
        cp.start()

    norm_gain = jnp.concatenate([nsc[i : i + 1, :] for i in range(16)], axis=1).astype(f32)
    lt.wait()

    def norm_rows(i, _):
        rows = pl.ds(pl.multiple_of(i * 32, 32), 32)
        v = tok[rows, :].astype(f32)
        v = v * lax.rsqrt(jnp.mean(v * v, axis=1, keepdims=True) + eps) * norm_gain
        nrm[rows, :] = v.astype(bf16)
        return 0

    lax.fori_loop(0, 8, norm_rows, 0)

    r0, r1 = rt[0:1, :], rt[1:2, :]
    di = lax.broadcasted_iota(jnp.int32, (NEP, 256), 0)
    e_rel = jnp.zeros((NEP, 256), jnp.int32)
    for d in range(NEP):
        e_rel = jnp.where(di == d, ep_at(d, 1), e_rel)
    in0, in1 = e_rel == r0, e_rel == r1
    routed = in0 | in1
    onehot = jnp.where(routed, 1.0, 0.0).astype(bf16)
    a = lax.broadcasted_iota(jnp.int32, (256, 256), 0)
    b = lax.broadcasted_iota(jnp.int32, (256, 256), 1)
    before = jnp.where(a < b, 1.0, 0.0).astype(bf16)
    place = jnp.dot(onehot, before, preferred_element_type=f32)
    place = jnp.where(routed, place, -1.0)
    slot = lax.broadcasted_iota(jnp.int32, (HALF, 256), 0) + HALF * c
    slot = slot.astype(f32)
    tokens_n = nrm[...]
    for q in range(4):
        pick = jnp.concatenate(
            [jnp.where(place[d : d + 1, :] == slot, 1.0, 0.0) for d in range(4 * q, 4 * q + 4)], axis=0
        ).astype(bf16)
        sbuf[q * 128 : (q + 1) * 128, :] = jnp.dot(pick, tokens_n, preferred_element_type=f32).astype(bf16)
    pl.semaphore_wait(barrier, NEP - 1 + NZ - 1 + 1)
    after = (ep + 1) % NEP
    halo = [
        push(u_h.at[tail, :], ub.at[pl.ds(0, 8), :], hl_s.at[0], hh_s.at[0], after, tp),
        push(bm_h.at[tail, map_cols], bb.at[pl.ds(0, 8), :], hl_s.at[1], hh_s.at[1], after, tp),
        push(cm_h.at[tail, map_cols], cb.at[pl.ds(0, 8), :], hl_s.at[2], hh_s.at[2], after, tp),
    ]
    for cp in halo:
        cp.start()

    dn_r = [
        push(down_cols(q, 1 - c), dn.at[c, :, pl.ds(q * 128, 128)], dns_s.at[q], dnr_s.at[q], ep, other)
        for q in range(NZ)
    ]
    for cp in dn_r:
        cp.start()
    def w_copy(way, k, part):
        if way == 0:
            a, b, t = (9 - k) % NZ, NZ - k, tp_at(1)
        else:
            a, b, t = k - 1, k, tp_at(NZ - 1)
        lo = 64 * part
        src = w_h.at[pl.ds(lo, 64), :] if k == 1 else wg.at[pl.ds(a * 128 + lo, 64), :]
        return push(
            src, wg.at[pl.ds(b * 128 + lo, 64), :],
            ws_s.at[way, part, k - 1], wr_s.at[way, part, k - 1], ep, t,
        )

    w_cp = {
        (way, k, part): w_copy(way, k, part)
        for way in range(2) for k in range(1, 5) for part in range(2)
        if k < 4 or part == way
    }

    def w_step(k, part):
        for way in range(2):
            if (way, k, part) in w_cp:
                if k > 1:
                    w_cp[way, k - 1, part].wait_recv()
                w_cp[way, k, part].start()

    w_step(1, 0)
    w_step(1, 1)

    x_cp = [
        push(
            sbuf.at[pl.ds(d * HALF, HALF), :],
            xr.at[pl.ds(pl.multiple_of(d * CAP + HALF * c, HALF), HALF), :],
            xs_s.at[d], xr_s.at[d], ep_at(d, 1), tp,
        )
        for d in range(1, NEP)
    ]
    for cp in x_cp[:EARLY]:
        cp.start()
    xr[pl.ds(pl.multiple_of(HALF * c, HALF), HALF), :] = sbuf[0:HALF, :]

    nt = (((1,), (1,)), ((), ()))
    gl = lax.dot_general(rg[...], tokens_n, nt, preferred_element_type=f32)
    el = lax.dot_general(re[...], tokens_n, nt, preferred_element_type=f32)

    def lse(v):
        top = jnp.max(v, axis=0, keepdims=True)
        return top + jnp.log(jnp.sum(jnp.exp(v - top), axis=0, keepdims=True))

    gl = gl - lse(gl)
    ei = lax.broadcasted_iota(jnp.int32, (4, 256), 0)
    lp0 = jnp.zeros((1, 256), f32)
    lp1 = jnp.zeros((1, 256), f32)
    for g in range(4):
        part = el[4 * g : 4 * g + 4, :]
        part = part - lse(part) + gl[g : g + 1, :]
        lp0 += jnp.sum(jnp.where(ei + 4 * g == r0, part, 0.0), axis=0, keepdims=True)
        lp1 += jnp.sum(jnp.where(ei + 4 * g == r1, part, 0.0), axis=0, keepdims=True)
    top = jnp.maximum(lp0, lp1)
    w0, w1 = jnp.exp(lp0 - top), jnp.exp(lp1 - top)
    total = w0 + w1
    share = jnp.where(in0, w0 / total, 0.0) + jnp.where(in1, w1 / total, 0.0)
    both = jnp.concatenate([place, share, jnp.zeros((96, 256), f32)], axis=0).T

    lane = lax.broadcasted_iota(jnp.int32, (256, 128), 1)
    in_slot = (lane & (CAP - 1)).astype(f32)
    low = lane < CAP
    mixw = []
    for p in range(8):
        at = jnp.where(low, both[:, 2 * p : 2 * p + 1], both[:, 2 * p + 1 : 2 * p + 2])
        sh = jnp.where(low, both[:, 16 + 2 * p : 17 + 2 * p], both[:, 17 + 2 * p : 18 + 2 * p])
        mixw.append(jnp.where(at == in_slot, sh, 0.0).astype(bf16))
    mixw = jnp.concatenate(mixw, axis=1)

    row = lax.broadcasted_iota(jnp.int32, (32, 128), 0)
    lane1 = lax.broadcasted_iota(jnp.int32, (1, 128), 1)
    first = lax.broadcasted_iota(jnp.int32, (128, 128), 1) < 64
    at_l = lax.broadcasted_iota(jnp.int32, (128, 128), 0)
    at_s = lax.broadcasted_iota(jnp.int32, (128, 128), 1)
    lower = at_l >= at_s
    sv = sl[...]
    dt = jnp.maximum(sv, 0.0) + jnp.log1p(jnp.exp(-jnp.abs(sv)))
    speed = jnp.exp(jnp.where((row & 1) == 0, rate[0], rate[1]))
    log_decay = ex[...] - dt * speed
    upto = jnp.where(at_l <= at_s, 1.0, 0.0).astype(f32)
    cum = jnp.dot(log_decay, upto, precision=exact_prec, preferred_element_type=f32)
    cumr[...] = cum
    dtr[...] = dt
    turned = jnp.concatenate([cum, dt, jnp.zeros((64, 128), f32)], axis=0).T
    for b in range(16):
        rows = slice(128 * b, 128 * (b + 1))
        c0l[rows, :] = jnp.broadcast_to(turned[:, 2 * b : 2 * b + 1], (128, 128))
        c1l[rows, :] = jnp.broadcast_to(turned[:, 2 * b + 1 : 2 * b + 2], (128, 128))
        dtl[rows, :] = jnp.where(first, turned[:, 32 + 2 * b : 33 + 2 * b], turned[:, 33 + 2 * b : 34 + 2 * b])

    for cp in l_mix:
        cp.wait()
    for cp in halo:
        cp.wait_recv()
    for buf in (ub, bb, cb):
        edge = buf[0:8, :]
        buf[0:8, :] = jnp.where(ep == 0, jnp.zeros_like(edge), edge)
    tap_u = ut[...].astype(f32)
    block_0 = grp // 2 == 0
    tap_b = jnp.where(block_0, bt[:, 0:128].astype(f32), bt[:, 128:256].astype(f32))
    tap_c = jnp.where(block_0, ct[:, 0:128].astype(f32), ct[:, 128:256].astype(f32))
    own_half = (lane1 // 64) == grp % 2

    def conv(buf, taps, base):
        ext = buf[pl.ds(base, 136), :].astype(f32)
        tot = taps[0:1, :] * ext[5:133, :]
        for j in range(1, 4):
            tot += taps[j : j + 1, :] * ext[5 + j : 133 + j, :]
        return tot * jax.nn.sigmoid(tot)

    def one_block(b, carry):
        state, since = carry
        base = pl.multiple_of(b * 128, 128)
        rows = pl.ds(base, 128)
        xs = conv(ub, tap_u, base).astype(bf16)
        bs = conv(bb, tap_b, base).astype(bf16)
        cs = jnp.where(own_half, conv(cb, tap_c, base), 0.0).astype(bf16)
        xsb[rows, :] = xs
        csb[rows, :] = cs
        tst[pl.ds(b, 1), :] = since
        scores = lax.dot_general(cs, bs, (((1,), (1,)), ((), ())), preferred_element_type=f32)
        inner = []
        for h, col in ((0, c0l), (1, c1l)):
            at = pl.ds(2 * b + h, 1)
            diff = jnp.where(lower, col[rows, :] - cumr[at, :], 0.0)
            near = jnp.where(lower, scores * jnp.exp(diff) * dtr[at, :], 0.0).astype(bf16)
            inner.append(jnp.dot(near, xs, preferred_element_type=f32))
        both_cum = jnp.where(first, c0l[rows, :], c1l[rows, :])
        carried = jnp.dot(cs, state.astype(bf16), preferred_element_type=f32) * jnp.exp(both_cum)
        ssm[rows, :] = jnp.where(first, inner[0], inner[1]) + carried
        last = both_cum[127:128, :]
        weighed = (xs.astype(f32) * (jnp.exp(last - both_cum) * dtl[rows, :])).astype(bf16)
        gained = lax.dot_general(bs, weighed, (((0,), (0,)), ((), ())), preferred_element_type=f32)
        return state * jnp.exp(last) + gained, since + last

    carry = lax.fori_loop(
        0, 8, one_block, (jnp.zeros((128, 128), f32), jnp.zeros((1, 128), f32))
    )
    w_step(2, 0)
    state, since = lax.fori_loop(8, 16, one_block, carry)
    spad[...] = state
    half_rows = pl.ds(pl.multiple_of((grp % 2) * 64, 64), 64)
    ssend[0:64, :] = spad[half_rows, :].astype(bf16)
    decay = jnp.exp(since)
    near_decay = decay.astype(bf16)
    rest_decay = (decay - near_decay.astype(f32)).astype(bf16)
    row8 = lax.broadcasted_iota(jnp.int32, (8, 128), 0)
    ssend[64:72, :] = jnp.where(
        row8 == 0, near_decay.astype(f32), jnp.where(row8 == 1, rest_decay.astype(f32), 0.0)
    ).astype(bf16)
    s_cp = [
        push(ssend, sst.at[ep], ss_s.at[d], sr_s.at[d], ep_at(d, 1), tp) for d in range(1, NEP)
    ]
    for cp in s_cp:
        cp.start()
    for cp in x_cp[EARLY:]:
        cp.start()
    w_step(2, 1)


    def mixer_rest():
        for cp in s_cp:
            cp.wait_recv()

        def chain(j, ent):
            got = sst[j].astype(f32)
            return jnp.where(j < ep, ent * (got[64:65, :] + got[65:66, :]) + got[0:64, :], ent)

        ent = lax.fori_loop(0, NEP - 1, chain, jnp.zeros((64, 128), f32))
        entb[...] = jnp.zeros_like(entb)
        entb[half_rows, :] = ent.astype(bf16)
        scale = jnp.where(lane1 < 64, direct[0], direct[1])
        gain = gn[...].astype(f32)

        def rows_of(j, keep):
            for k in range(2):
                b = 2 * j + k
                rows = pl.ds(pl.multiple_of(b * 128, 128), 128)
                since_b = jnp.where(first, c0l[rows, :], c1l[rows, :]) + tst[pl.ds(b, 1), :]
                far = jnp.dot(csb[rows, :], entb[...], preferred_element_type=f32) * jnp.exp(since_b)
                gate = ogb[rows, :].astype(f32)
                val = (ssm[rows, :] + far + scale * xsb[rows, :].astype(f32)) * (gate * jax.nn.sigmoid(gate))
                sq = val * val
                sum0 = jnp.sum(jnp.where(first, sq, 0.0), axis=1, keepdims=True)
                sum1 = jnp.sum(jnp.where(first, 0.0, sq), axis=1, keepdims=True)
                ms = jnp.where(first, sum0, sum1) * (1.0 / 64)
                keep(k, rows, (val * lax.rsqrt(ms + eps) * gain).astype(bf16))

        def send_on(i, _):
            j = (z + 1 + i) % NZ

            def keep(k, rows, val):
                mixb[rows, :] = val

            rows_of(j, keep)
            push(
                mixb.at[pl.ds(pl.multiple_of(j * 256, 256), 256), :],
                mx.at[:, pl.ds(pl.multiple_of((7 - i) * 128, 128), 128)],
                ms_s.at[7 - i], mr_s.at[7 - i], ep, tp_at(1 + i),
            ).start()
            return 0

        lax.fori_loop(0, NZ - 1, send_on, 0)

        def own(k, rows, val):
            mx[128 * k : 128 * (k + 1), 0:128] = val

        rows_of(z, own)

    m_cp = [
        push(
            mixb.at[pl.ds(pl.multiple_of(((z + r) % NZ) * 256, 256), 256), :],
            mx.at[:, pl.ds((NZ - r) * 128, 128)],
            ms_s.at[NZ - r], mr_s.at[NZ - r], ep, tp_at(r),
        )
        for r in range(1, NZ)
    ]

    lg.wait()
    lu.wait()
    for cp in dn_l:
        cp.wait()

    def x_hand(d):
        rows = pl.ds(pl.multiple_of(d * CAP + HALF * c, HALF), HALF)
        return push(xr.at[rows, :], xr.at[rows, :], xf_s.at[d], xg_s.at[d], ep, other)

    hand = [x_hand(d) for d in range(NEP)]

    def y_copy(d, h):
        part = (pl.ds(d * CAP, CAP), pl.ds(h * 512, 512))
        return push(ysend.at[part], ybuf.at[part], ys_s.at[h, d], yr_s.at[h, d], ep_at(d, -1), tp)

    y_cp = [[y_copy(d, h) for d in range(1, NEP)] for h in range(2)]
    h_cp = []
    for g in range(4):
        for d in range(4 * g, 4 * g + 4):
            if d > 0:
                x_cp[d - 1].wait_recv()
            hand[d].start()
        for d in range(4 * g, 4 * g + 4):
            hand[d].wait_recv()
        rows = slice(256 * g, 256 * (g + 1))
        xg = xr[rows, :]
        gv = jnp.dot(xg, gw[...], preferred_element_type=f32)
        uv = jnp.dot(xg, uw[...], preferred_element_type=f32)
        hall[c, rows, :] = (gv * jax.nn.sigmoid(gv) * uv).astype(bf16)
        part = hall.at[c, pl.ds(256 * g, 256), :]
        cp = push(part, part, hs_s.at[g], hr_s.at[g], ep, other)
        cp.start()
        h_cp.append(cp)
        if g == 0:
            for cq in dn_r:
                cq.wait_recv()
        if g == 0:
            w_step(3, 0)
        if g == 2:
            w_step(4, 0)
            w_step(4, 1)
            mixer_rest()
        cp.wait_recv()
        yv = jnp.dot(hall[0, rows, :], dn[0], preferred_element_type=f32)
        yv += jnp.dot(hall[1, rows, :], dn[1], preferred_element_type=f32)
        ysend[rows, :] = yv.astype(bf16)
        for d in range(4 * g, 4 * g + 4):
            if d > 0:
                y_cp[0][d - 1].start()
        if g == 1:
            w_step(3, 1)
    for d in range(1, NEP):
        y_cp[1][d - 1].start()
    ybuf[0:CAP, :] = ysend[0:CAP, :]

    def project():
        lw.wait()
        for cp in m_cp:
            cp.wait_recv()
        for way in range(2):
            w_cp[way, 3, 1 - way].wait_recv()
            w_cp[way, 4, way].wait_recv()
        theirs = mx[pl.ds(pl.multiple_of((1 - c) * 128, 128), 128), :]
        psend[...] = jnp.dot(theirs, wg[...], preferred_element_type=f32).astype(bf16)
        fin = push(psend, precv, fs_s, fr_s, ep, other)
        fin.start()
        ours = mx[pl.ds(pl.multiple_of(c * 128, 128), 128), :]
        mine = jnp.dot(ours, wg[...], preferred_element_type=f32)
        keep_mine[...] = mine
        return fin

    z_cp = []
    for h in range(2):
        for d in range(1, NEP):
            y_cp[h][d - 1].wait_recv()
        cols = slice(512 * h, 512 * (h + 1))
        comb = jnp.dot(mixw, ybuf[:, cols], preferred_element_type=f32)
        for i in range(4):
            r = ORDER[4 * h + i]
            val = comb[:, 128 * i : 128 * (i + 1)]
            if r == 0:
                zbuf[0] = val.astype(bf16)
                continue
            zsend[r] = val.astype(bf16)
            cp = push(zsend.at[r], zbuf.at[NZ - r], zs_s.at[NZ - r], zr_s.at[NZ - r], ep, tp_at(r))
            cp.start()
            z_cp.append(cp)
        if h == 0:
            fin = project()

    fin.wait_recv()
    mo[...] = (keep_mine[...] + precv[...].astype(f32)).astype(bf16)

    acc = zbuf[0].astype(f32)
    for cp in z_cp:
        cp.wait_recv()
    for r in range(1, NZ):
        acc += zbuf[r].astype(f32)
    eo[...] = acc.astype(bf16)

    for cp in dn_r + m_cp + x_cp + halo + s_cp + hand + y_cp[0] + y_cp[1] + h_cp + z_cp + [fin]:
        cp.wait_send()
    for cp in w_cp.values():
        cp.wait_send()


def fused(*args):
    vmem, hbm = pl.BlockSpec(memory_space=pltpu.VMEM), pl.BlockSpec(memory_space=pl.ANY)
    smem = pl.BlockSpec(memory_space=pltpu.SMEM)
    dma = pltpu.SemaphoreType.DMA
    v = pltpu.VMEM
    return pl.pallas_call(
        kernel,
        out_shape=(
            pltpu.VMEM((128, 2048), bf16),
            pltpu.VMEM((256, 128), bf16),
        ),
        in_specs=[vmem] * 10 + [smem] * 2 + [hbm] * 9,
        out_specs=(vmem, vmem),
        scratch_shapes=[
            v((256, 2048), bf16),
            v((512, 2048), bf16),
            v((1024, 2048), bf16),
            v((2048, 256), bf16),
            v((2048, 256), bf16),
            v((2, 256, 1024), bf16),
            v((2, 1024, 256), bf16),
            v((1024, 1024), bf16),
            v((1024, 1024), bf16),
            v((8, 256, 128), bf16),
            v((8, 256, 128), bf16),
            v((1024, 2048), bf16),
            v((256, 1024), bf16),
            v((128, 2048), bf16),
            v((128, 2048), bf16),
            v((2056, 128), bf16),
            v((2056, 128), bf16),
            v((2056, 128), bf16),
            v((2048, 128), bf16),
            v((2048, 128), bf16),
            v((2048, 128), bf16),
            v((2048, 128), f32),
            v((2048, 128), f32),
            v((2048, 128), f32),
            v((32, 128), f32),
            v((32, 128), f32),
            v((16, 128), f32),
            v((2048, 128), f32),
            v((128, 128), f32),
            v((72, 128), bf16),
            v((16, 72, 128), bf16),
            v((128, 128), bf16),
            v((2048, 128), bf16),
            v((128, 2048), f32),
            v((256, 2048), bf16),
            dma((8,)), dma((8,)), dma((8,)), dma((8,)),
            dma((16,)), dma((16,)), dma((16,)), dma((16,)),
            dma((4,)), dma((4,)), dma((2, 16)), dma((2, 16)),
            dma((8,)), dma((8,)), dma((2, 2, 4)), dma((2, 2, 4)), dma((8,)), dma((8,)),
            dma, dma, dma((3,)), dma((3,)), dma((16,)), dma((16,)),
        ],
        compiler_params=pltpu.CompilerParams(
            collective_id=0, has_side_effects=True, vmem_limit_bytes=56 * 1024 * 1024
        ),
    )(*args)


def per_device(
    mixer_input_channels,
    output_gate_logits,
    head_group_input_map,
    head_group_output_map,
    input_channel_taps,
    input_map_taps,
    output_map_taps,
    step_logits,
    head_log_rate,
    extra_log_decay,
    head_direct_scale,
    gated_norm_scale,
    mixer_output_weight,
    second_batch_tokens,
    pre_expert_norm_scale,
    group_router_columns,
    expert_router_columns,
    routes,
    expert_gate_weight,
    expert_up_weight,
    expert_down_weight,
):
    def by_block(v):
        return jnp.transpose(v.reshape(2, 16, 128), (1, 0, 2)).reshape(32, 128)

    return fused(
        pre_expert_norm_scale.reshape(16, 128),
        group_router_columns.T,
        expert_router_columns.T,
        routes.T,
        input_channel_taps,
        input_map_taps,
        output_map_taps,
        by_block(step_logits),
        by_block(extra_log_decay),
        gated_norm_scale.reshape(1, -1),
        head_log_rate,
        head_direct_scale,
        second_batch_tokens,
        expert_gate_weight[0],
        expert_up_weight[0],
        expert_down_weight[0],
        mixer_output_weight,
        mixer_input_channels,
        output_gate_logits,
        head_group_input_map,
        head_group_output_map,
    )


def solution(mesh):
    in_specs = (
        P("ep", "tp"),
        P("ep", "tp"),
        P("ep", None),
        P("ep", None),
        P(None, "tp"),
        P(),
        P(),
        P("tp", "ep"),
        P("tp"),
        P("tp", "ep"),
        P("tp"),
        P("tp"),
        P("tp", None),
        P("ep", None),
        P(),
        P(),
        P(),
        P("ep", None),
        P("ep", None, "tp"),
        P("ep", None, "tp"),
        P("ep", "tp", None),
    )
    out_specs = (P(("ep", "tp"), None), P("ep", "tp"))
    return jax.shard_map(
        per_device, mesh=mesh, in_specs=in_specs, out_specs=out_specs, check_vma=False
    )
```

```python
import jax
import jax.numpy as jnp
from jax import lax
from jax.experimental import pallas as pl
from jax.experimental.pallas import tpu as pltpu
from jax.sharding import PartitionSpec as P

eps = 1e-06
exact_prec = lax.Precision.HIGHEST
bf16, f32 = jnp.bfloat16, jnp.float32

NEP = 16
NZ = 8
CAP = 64
HALF = CAP // 2
ORDER = (4, 3, 5, 1, 2, 6, 7, 0)
NEAR = (
    (0, 0), (1, 0), (0, 1), (3, 0), (0, 3), (1, 1), (3, 3), (1, 3),
    (3, 1), (2, 0), (0, 2), (2, 1), (1, 2), (3, 2), (2, 3), (2, 2),
)
EARLY = 16


def kernel(
    nsc_h, rg_h, re_h, rt_h, ut_h, bt_h, ct_h, sl_h, ex_h, gn_h, rate, direct,
    tok_h, gate_h, up_h, down_h, w_h, u_h, og_h, bm_h, cm_h,
    mo, eo,
    nrm, sbuf, xr, gw, uw, dn, hall, ysend, ybuf, zsend, zbuf, wg, mx, psend, precv,
    ub, bb, cb, ogb, xsb, csb, c0l, c1l, dtl, cumr, dtr, tst, ssm, spad, ssend, sst, entb, mixb, keep_mine, tok, zway, zown,
    nsc, rg, re, rt, ut, bt, ct, sl, ex, gn, small_s,
    loc_s, dnl_s, dns_s, dnr_s, xs_s, xr_s, xf_s, xg_s, hs_s, hr_s, ys_s, yr_s, zs_s, zr_s,
    ws_s, wr_s, ms_s, mr_s, fs_s, fr_s, hl_s, hh_s, ss_s, sr_s, zws_s, zwr_s,
):
    ep, tp = lax.axis_index("ep"), lax.axis_index("tp")
    y, x = ep // 4, ep % 4
    z, c = tp // 2, tp % 2
    other = z * 2 + (1 - c)

    def ep_at(d, sign):
        dx, dy = NEAR[d]
        return ((y + 4 + sign * dy) % 4) * 4 + (x + 4 + sign * dx) % 4

    def tp_at(r):
        return ((z + r) % NZ) * 2 + c

    def push(src, dst, ss, rs, e, t):
        return pltpu.make_async_remote_copy(
            src_ref=src, dst_ref=dst, send_sem=ss, recv_sem=rs,
            device_id={"ep": e, "tp": t}, device_id_type=pl.DeviceIdType.MESH,
        )

    barrier = pltpu.get_barrier_semaphore()

    def greet(e, t):
        pl.semaphore_signal(
            barrier, inc=1, device_id={"ep": e, "tp": t}, device_id_type=pl.DeviceIdType.MESH
        )

    for d in range(1, NEP):
        greet(ep_at(d, 1), tp)
    for r in range(1, NZ):
        greet(ep, tp_at(r))
    greet(ep, other)

    small = [
        pltpu.make_async_copy(src, dst, small_s.at[i])
        for i, (src, dst) in enumerate((
            (rt_h, rt), (nsc_h, nsc), (rg_h, rg), (re_h, re), (ut_h, ut), (bt_h, bt),
            (ct_h, ct), (sl_h, sl), (ex_h, ex), (gn_h, gn),
        ))
    ]
    for cp in small[:2]:
        cp.start()
    lt = pltpu.make_async_copy(tok_h, tok, loc_s.at[7])
    lt.start()
    for cp in small[2:]:
        cp.start()
    lg = pltpu.make_async_copy(gate_h, gw, loc_s.at[0])
    lu = pltpu.make_async_copy(up_h, uw, loc_s.at[1])
    lw = pltpu.make_async_copy(w_h, wg.at[pl.ds(0, 128), :], loc_s.at[2])
    grp = tp // 4
    map_cols = pl.ds(pl.multiple_of((grp // 2) * 128, 128), 128)
    body, tail = pl.ds(8, 2048), pl.ds(2040, 8)
    l_mix = [
        pltpu.make_async_copy(u_h, ub.at[body, :], loc_s.at[4]),
        pltpu.make_async_copy(bm_h.at[:, map_cols], bb.at[body, :], loc_s.at[5]),
        pltpu.make_async_copy(cm_h.at[:, map_cols], cb.at[body, :], loc_s.at[6]),
        pltpu.make_async_copy(og_h, ogb, loc_s.at[3]),
    ]
    for cp in l_mix + [lg, lu, lw]:
        cp.start()

    def down_cols(q, core):
        return down_h.at[:, pl.ds(pl.multiple_of((2 * ((z + ORDER[q]) % NZ) + core) * 128, 128), 128)]

    dn_l = [
        pltpu.make_async_copy(
            down_cols(q, c), dn.at[c, :, pl.ds(q * 128, 128)], dnl_s.at[q]
        )
        for q in range(NZ)
    ]
    for cp in dn_l:
        cp.start()

    for cp in small:
        cp.wait()
    norm_gain = jnp.concatenate([nsc[i : i + 1, :] for i in range(16)], axis=1).astype(f32)
    lt.wait()

    def norm_rows(i, _):
        rows = pl.ds(pl.multiple_of(i * 32, 32), 32)
        v = tok[rows, :].astype(f32)
        v = v * lax.rsqrt(jnp.mean(v * v, axis=1, keepdims=True) + eps) * norm_gain
        nrm[rows, :] = v.astype(bf16)
        return 0

    lax.fori_loop(0, 8, norm_rows, 0)

    r0, r1 = rt[0:1, :], rt[1:2, :]
    di = lax.broadcasted_iota(jnp.int32, (NEP, 256), 0)
    e_rel = jnp.zeros((NEP, 256), jnp.int32)
    for d in range(NEP):
        e_rel = jnp.where(di == d, ep_at(d, 1), e_rel)
    in0, in1 = e_rel == r0, e_rel == r1
    routed = in0 | in1
    onehot = jnp.where(routed, 1.0, 0.0).astype(bf16)
    a = lax.broadcasted_iota(jnp.int32, (256, 256), 0)
    b = lax.broadcasted_iota(jnp.int32, (256, 256), 1)
    before = jnp.where(a < b, 1.0, 0.0).astype(bf16)
    place = jnp.dot(onehot, before, preferred_element_type=f32)
    place = jnp.where(routed, place, -1.0)
    slot = lax.broadcasted_iota(jnp.int32, (HALF, 256), 0) + HALF * c
    slot = slot.astype(f32)
    tokens_n = nrm[...]
    for q in range(4):
        pick = jnp.concatenate(
            [jnp.where(place[d : d + 1, :] == slot, 1.0, 0.0) for d in range(4 * q, 4 * q + 4)], axis=0
        ).astype(bf16)
        sbuf[q * 128 : (q + 1) * 128, :] = jnp.dot(pick, tokens_n, preferred_element_type=f32).astype(bf16)
    pl.semaphore_wait(barrier, NEP - 1 + NZ - 1 + 1)
    after = (ep + 1) % NEP
    halo = [
        push(u_h.at[tail, :], ub.at[pl.ds(0, 8), :], hl_s.at[0], hh_s.at[0], after, tp),
        push(bm_h.at[tail, map_cols], bb.at[pl.ds(0, 8), :], hl_s.at[1], hh_s.at[1], after, tp),
        push(cm_h.at[tail, map_cols], cb.at[pl.ds(0, 8), :], hl_s.at[2], hh_s.at[2], after, tp),
    ]
    for cp in halo:
        cp.start()

    dn_r = [
        push(down_cols(q, 1 - c), dn.at[c, :, pl.ds(q * 128, 128)], dns_s.at[q], dnr_s.at[q], ep, other)
        for q in range(NZ)
    ]
    for cp in dn_r:
        cp.start()
    def w_copy(way, k, part):
        if way == 0:
            a, b, t = (9 - k) % NZ, NZ - k, tp_at(1)
        else:
            a, b, t = k - 1, k, tp_at(NZ - 1)
        lo = 64 * part
        src = w_h.at[pl.ds(lo, 64), :] if k == 1 else wg.at[pl.ds(a * 128 + lo, 64), :]
        return push(
            src, wg.at[pl.ds(b * 128 + lo, 64), :],
            ws_s.at[way, part, k - 1], wr_s.at[way, part, k - 1], ep, t,
        )

    w_cp = {
        (way, k, part): w_copy(way, k, part)
        for way in range(2) for k in range(1, 5) for part in range(2)
        if k < 4 or part == way
    }

    def w_step(k, part):
        for way in range(2):
            if (way, k, part) in w_cp:
                if k > 1:
                    w_cp[way, k - 1, part].wait_recv()
                w_cp[way, k, part].start()

    w_step(1, 0)
    w_step(1, 1)

    x_cp = [
        push(
            sbuf.at[pl.ds(d * HALF, HALF), :],
            xr.at[pl.ds(pl.multiple_of(d * CAP + HALF * c, HALF), HALF), :],
            xs_s.at[d], xr_s.at[d], ep_at(d, 1), tp,
        )
        for d in range(1, NEP)
    ]
    for cp in x_cp[:EARLY]:
        cp.start()
    xr[pl.ds(pl.multiple_of(HALF * c, HALF), HALF), :] = sbuf[0:HALF, :]

    def x_hand(d):
        rows = pl.ds(pl.multiple_of(d * CAP + HALF * c, HALF), HALF)
        return push(xr.at[rows, :], xr.at[rows, :], xf_s.at[d], xg_s.at[d], ep, other)

    hand = [x_hand(d) for d in range(NEP)]

    def pass_on(g):
        for d in range(4 * g, 4 * g + 4):
            if d > 0:
                x_cp[d - 1].wait_recv()
            hand[d].start()

    nt = (((1,), (1,)), ((), ()))
    gl = lax.dot_general(rg[...], tokens_n, nt, preferred_element_type=f32)
    el = lax.dot_general(re[...], tokens_n, nt, preferred_element_type=f32)

    def lse(v):
        top = jnp.max(v, axis=0, keepdims=True)
        return top + jnp.log(jnp.sum(jnp.exp(v - top), axis=0, keepdims=True))

    gl = gl - lse(gl)
    ei = lax.broadcasted_iota(jnp.int32, (4, 256), 0)
    lp0 = jnp.zeros((1, 256), f32)
    lp1 = jnp.zeros((1, 256), f32)
    for g in range(4):
        part = el[4 * g : 4 * g + 4, :]
        part = part - lse(part) + gl[g : g + 1, :]
        lp0 += jnp.sum(jnp.where(ei + 4 * g == r0, part, 0.0), axis=0, keepdims=True)
        lp1 += jnp.sum(jnp.where(ei + 4 * g == r1, part, 0.0), axis=0, keepdims=True)
    top = jnp.maximum(lp0, lp1)
    w0, w1 = jnp.exp(lp0 - top), jnp.exp(lp1 - top)
    total = w0 + w1
    share = jnp.where(in0, w0 / total, 0.0) + jnp.where(in1, w1 / total, 0.0)
    both = jnp.concatenate([place, share, jnp.zeros((96, 256), f32)], axis=0).T

    lane = lax.broadcasted_iota(jnp.int32, (256, 128), 1)
    in_slot = (lane & (CAP - 1)).astype(f32)
    low = lane < CAP
    mixw = []
    for p in range(8):
        at = jnp.where(low, both[:, 2 * p : 2 * p + 1], both[:, 2 * p + 1 : 2 * p + 2])
        sh = jnp.where(low, both[:, 16 + 2 * p : 17 + 2 * p], both[:, 17 + 2 * p : 18 + 2 * p])
        mixw.append(jnp.where(at == in_slot, sh, 0.0).astype(bf16))
    mixw = jnp.concatenate(mixw, axis=1)

    row = lax.broadcasted_iota(jnp.int32, (32, 128), 0)
    lane1 = lax.broadcasted_iota(jnp.int32, (1, 128), 1)
    first = lax.broadcasted_iota(jnp.int32, (128, 128), 1) < 64
    at_l = lax.broadcasted_iota(jnp.int32, (128, 128), 0)
    at_s = lax.broadcasted_iota(jnp.int32, (128, 128), 1)
    lower = at_l >= at_s
    sv = sl[...]
    dt = jnp.maximum(sv, 0.0) + jnp.log1p(jnp.exp(-jnp.abs(sv)))
    speed = jnp.exp(jnp.where((row & 1) == 0, rate[0], rate[1]))
    log_decay = ex[...] - dt * speed
    upto = jnp.where(at_l <= at_s, 1.0, 0.0).astype(f32)
    cum = jnp.dot(log_decay, upto, precision=exact_prec, preferred_element_type=f32)
    cumr[...] = cum
    dtr[...] = dt
    turned = jnp.concatenate([cum, dt, jnp.zeros((64, 128), f32)], axis=0).T
    for b in range(16):
        rows = slice(128 * b, 128 * (b + 1))
        c0l[rows, :] = jnp.broadcast_to(turned[:, 2 * b : 2 * b + 1], (128, 128))
        c1l[rows, :] = jnp.broadcast_to(turned[:, 2 * b + 1 : 2 * b + 2], (128, 128))
        dtl[rows, :] = jnp.where(first, turned[:, 32 + 2 * b : 33 + 2 * b], turned[:, 33 + 2 * b : 34 + 2 * b])

    for cp in l_mix:
        cp.wait()
    for cp in halo:
        cp.wait_recv()
    for buf in (ub, bb, cb):
        edge = buf[0:8, :]
        buf[0:8, :] = jnp.where(ep == 0, jnp.zeros_like(edge), edge)
    tap_u = ut[...].astype(f32)
    block_0 = grp // 2 == 0
    tap_b = jnp.where(block_0, bt[:, 0:128].astype(f32), bt[:, 128:256].astype(f32))
    tap_c = jnp.where(block_0, ct[:, 0:128].astype(f32), ct[:, 128:256].astype(f32))
    own_half = (lane1 // 64) == grp % 2

    def conv(buf, taps, base):
        ext = buf[pl.ds(base, 136), :].astype(f32)
        tot = taps[0:1, :] * ext[5:133, :]
        for j in range(1, 4):
            tot += taps[j : j + 1, :] * ext[5 + j : 133 + j, :]
        return tot * jax.nn.sigmoid(tot)

    def one_block(b, carry):
        state, since = carry
        base = pl.multiple_of(b * 128, 128)
        rows = pl.ds(base, 128)
        xs = conv(ub, tap_u, base).astype(bf16)
        bs = conv(bb, tap_b, base).astype(bf16)
        cs = jnp.where(own_half, conv(cb, tap_c, base), 0.0).astype(bf16)
        xsb[rows, :] = xs
        csb[rows, :] = cs
        tst[pl.ds(b, 1), :] = since
        scores = lax.dot_general(cs, bs, (((1,), (1,)), ((), ())), preferred_element_type=f32)
        inner = []
        for h, col in ((0, c0l), (1, c1l)):
            at = pl.ds(2 * b + h, 1)
            diff = jnp.where(lower, col[rows, :] - cumr[at, :], 0.0)
            near = jnp.where(lower, scores * jnp.exp(diff) * dtr[at, :], 0.0).astype(bf16)
            inner.append(jnp.dot(near, xs, preferred_element_type=f32))
        both_cum = jnp.where(first, c0l[rows, :], c1l[rows, :])
        carried = jnp.dot(cs, state.astype(bf16), preferred_element_type=f32) * jnp.exp(both_cum)
        ssm[rows, :] = jnp.where(first, inner[0], inner[1]) + carried
        last = both_cum[127:128, :]
        weighed = (xs.astype(f32) * (jnp.exp(last - both_cum) * dtl[rows, :])).astype(bf16)
        gained = lax.dot_general(bs, weighed, (((0,), (0,)), ((), ())), preferred_element_type=f32)
        return state * jnp.exp(last) + gained, since + last

    carry = lax.fori_loop(
        0, 8, one_block, (jnp.zeros((128, 128), f32), jnp.zeros((1, 128), f32))
    )
    w_step(2, 0)
    state, since = lax.fori_loop(8, 16, one_block, carry)
    spad[...] = state
    half_rows = pl.ds(pl.multiple_of((grp % 2) * 64, 64), 64)
    ssend[0:64, :] = spad[half_rows, :].astype(bf16)
    decay = jnp.exp(since)
    near_decay = decay.astype(bf16)
    rest_decay = (decay - near_decay.astype(f32)).astype(bf16)
    row8 = lax.broadcasted_iota(jnp.int32, (8, 128), 0)
    ssend[64:72, :] = jnp.where(
        row8 == 0, near_decay.astype(f32), jnp.where(row8 == 1, rest_decay.astype(f32), 0.0)
    ).astype(bf16)
    s_cp = [
        push(ssend, sst.at[ep], ss_s.at[d], sr_s.at[d], ep_at(d, 1), tp) for d in range(1, NEP)
    ]
    for cp in s_cp:
        cp.start()
    for cp in x_cp[EARLY:]:
        cp.start()
    w_step(2, 1)


    def mixer_rest():
        for cp in s_cp:
            cp.wait_recv()

        def chain(j, ent):
            got = sst[j].astype(f32)
            return jnp.where(j < ep, ent * (got[64:65, :] + got[65:66, :]) + got[0:64, :], ent)

        ent = lax.fori_loop(0, NEP - 1, chain, jnp.zeros((64, 128), f32))
        entb[...] = jnp.zeros_like(entb)
        entb[half_rows, :] = ent.astype(bf16)
        scale = jnp.where(lane1 < 64, direct[0], direct[1])
        gain = gn[...].astype(f32)

        def rows_of(j, keep):
            for k in range(2):
                b = 2 * j + k
                rows = pl.ds(pl.multiple_of(b * 128, 128), 128)
                since_b = jnp.where(first, c0l[rows, :], c1l[rows, :]) + tst[pl.ds(b, 1), :]
                far = jnp.dot(csb[rows, :], entb[...], preferred_element_type=f32) * jnp.exp(since_b)
                gate = ogb[rows, :].astype(f32)
                val = (ssm[rows, :] + far + scale * xsb[rows, :].astype(f32)) * (gate * jax.nn.sigmoid(gate))
                sq = val * val
                sum0 = jnp.sum(jnp.where(first, sq, 0.0), axis=1, keepdims=True)
                sum1 = jnp.sum(jnp.where(first, 0.0, sq), axis=1, keepdims=True)
                ms = jnp.where(first, sum0, sum1) * (1.0 / 64)
                keep(k, rows, (val * lax.rsqrt(ms + eps) * gain).astype(bf16))

        def send_on(i, _):
            j = (z + 1 + i) % NZ

            def keep(k, rows, val):
                mixb[rows, :] = val

            rows_of(j, keep)
            push(
                mixb.at[pl.ds(pl.multiple_of(j * 256, 256), 256), :],
                mx.at[:, pl.ds(pl.multiple_of((7 - i) * 128, 128), 128)],
                ms_s.at[7 - i], mr_s.at[7 - i], ep, tp_at(1 + i),
            ).start()
            return 0

        lax.fori_loop(0, NZ - 1, send_on, 0)

        def own(k, rows, val):
            mx[128 * k : 128 * (k + 1), 0:128] = val

        rows_of(z, own)

    m_cp = [
        push(
            mixb.at[pl.ds(pl.multiple_of(((z + r) % NZ) * 256, 256), 256), :],
            mx.at[:, pl.ds((NZ - r) * 128, 128)],
            ms_s.at[NZ - r], mr_s.at[NZ - r], ep, tp_at(r),
        )
        for r in range(1, NZ)
    ]

    lg.wait()
    lu.wait()
    for cp in dn_l:
        cp.wait()

    def y_copy(d, h):
        part = (pl.ds(d * CAP, CAP), pl.ds(h * 512, 512))
        return push(ysend.at[part], ybuf.at[part], ys_s.at[h, d], yr_s.at[h, d], ep_at(d, -1), tp)

    y_cp = [[y_copy(d, h) for d in range(1, NEP)] for h in range(2)]
    h_cp = []
    for g in range(4):
        part = hall.at[c, pl.ds(256 * g, 256), :]
        h_cp.append(push(part, part, hs_s.at[g], hr_s.at[g], ep, other))

    def hidden(g):
        for d in range(4 * g, 4 * g + 4):
            hand[d].wait_recv()
        rows = slice(256 * g, 256 * (g + 1))
        xg = xr[rows, :]
        gv = jnp.dot(xg, gw[...], preferred_element_type=f32)
        uv = jnp.dot(xg, uw[...], preferred_element_type=f32)
        hall[c, rows, :] = (gv * jax.nn.sigmoid(gv) * uv).astype(bf16)
        h_cp[g].start()

    def results(g):
        rows = slice(256 * g, 256 * (g + 1))
        h_cp[g].wait_recv()
        yv = jnp.dot(hall[0, rows, :], dn[0], preferred_element_type=f32)
        yv += jnp.dot(hall[1, rows, :], dn[1], preferred_element_type=f32)
        ysend[rows, :] = yv.astype(bf16)
        for d in range(4 * g, 4 * g + 4):
            if d > 0:
                y_cp[0][d - 1].start()

    pass_on(0)
    pass_on(1)
    hidden(0)
    hidden(1)
    for cq in dn_r:
        cq.wait_recv()
    w_step(3, 0)
    results(0)
    results(1)
    w_step(3, 1)
    pass_on(2)
    hidden(2)
    pass_on(3)
    results(2)
    hidden(3)
    results(3)
    for d in range(1, NEP):
        y_cp[1][d - 1].start()
    w_step(4, 0)
    w_step(4, 1)
    mixer_rest()
    ybuf[0:CAP, :] = ysend[0:CAP, :]

    def project():
        lw.wait()
        for cp in m_cp:
            cp.wait_recv()
        for way in range(2):
            w_cp[way, 3, 1 - way].wait_recv()
            w_cp[way, 4, way].wait_recv()
        theirs = mx[pl.ds(pl.multiple_of((1 - c) * 128, 128), 128), :]
        psend[...] = jnp.dot(theirs, wg[...], preferred_element_type=f32).astype(bf16)
        fin = push(psend, precv, fs_s, fr_s, ep, other)
        fin.start()
        ours = mx[pl.ds(pl.multiple_of(c * 128, 128), 128), :]
        mine = jnp.dot(ours, wg[...], preferred_element_type=f32)
        keep_mine[...] = mine
        return fin

    first_hop = {4: (2, 0), 3: (1, 1), 5: (7, 2)}
    z_cp, on_way = [], []
    for h in range(2):
        for d in range(1, NEP):
            y_cp[h][d - 1].wait_recv()
        cols = slice(512 * h, 512 * (h + 1))
        comb = jnp.dot(mixw, ybuf[:, cols], preferred_element_type=f32)
        for i in ((0, 1, 2, 3), (2, 3, 0, 1))[h]:
            r = ORDER[4 * h + i]
            if r == 2:
                for cp in on_way:
                    cp.wait_recv()
            val = comb[:, 128 * i : 128 * (i + 1)]
            if r == 0:
                zown[...] = val
                continue
            if r in first_hop:
                hop, place_w = first_hop[r]
                zsend[r] = val.astype(bf16)
                cp = push(zsend.at[r], zway.at[place_w], zws_s.at[place_w], zwr_s.at[place_w], ep, tp_at(hop))
                cp.start()
                on_way.append(cp)
                continue
            if r == 2:
                val = val + zway[0].astype(f32) + zway[1].astype(f32)
            if r == 6:
                val = val + zway[2].astype(f32)
            zsend[r] = val.astype(bf16)
            cp = push(zsend.at[r], zbuf.at[NZ - r], zs_s.at[NZ - r], zr_s.at[NZ - r], ep, tp_at(r))
            cp.start()
            z_cp.append(cp)

    fin = project()
    fin.wait_recv()
    mo[...] = (keep_mine[...] + precv[...].astype(f32)).astype(bf16)

    acc = zown[...]
    for cp in z_cp:
        cp.wait_recv()
    for r in (1, 2, 6, 7):
        acc += zbuf[r].astype(f32)
    eo[...] = acc.astype(bf16)

    for cp in dn_r + m_cp + x_cp + halo + s_cp + hand + y_cp[0] + y_cp[1] + h_cp + z_cp + on_way + [fin]:
        cp.wait_send()
    for cp in w_cp.values():
        cp.wait_send()


def fused(*args):
    vmem, hbm = pl.BlockSpec(memory_space=pltpu.VMEM), pl.BlockSpec(memory_space=pl.ANY)
    smem = pl.BlockSpec(memory_space=pltpu.SMEM)
    dma = pltpu.SemaphoreType.DMA
    v = pltpu.VMEM
    return pl.pallas_call(
        kernel,
        out_shape=(
            pltpu.VMEM((128, 2048), bf16),
            pltpu.VMEM((256, 128), bf16),
        ),
        in_specs=[hbm] * 10 + [smem] * 2 + [hbm] * 9,
        out_specs=(vmem, vmem),
        scratch_shapes=[
            v((256, 2048), bf16),
            v((512, 2048), bf16),
            v((1024, 2048), bf16),
            v((2048, 256), bf16),
            v((2048, 256), bf16),
            v((2, 256, 1024), bf16),
            v((2, 1024, 256), bf16),
            v((1024, 1024), bf16),
            v((1024, 1024), bf16),
            v((8, 256, 128), bf16),
            v((8, 256, 128), bf16),
            v((1024, 2048), bf16),
            v((256, 1024), bf16),
            v((128, 2048), bf16),
            v((128, 2048), bf16),
            v((2056, 128), bf16),
            v((2056, 128), bf16),
            v((2056, 128), bf16),
            v((2048, 128), bf16),
            v((2048, 128), bf16),
            v((2048, 128), bf16),
            v((2048, 128), f32),
            v((2048, 128), f32),
            v((2048, 128), f32),
            v((32, 128), f32),
            v((32, 128), f32),
            v((16, 128), f32),
            v((2048, 128), f32),
            v((128, 128), f32),
            v((72, 128), bf16),
            v((16, 72, 128), bf16),
            v((128, 128), bf16),
            v((2048, 128), bf16),
            v((128, 2048), f32),
            v((256, 2048), bf16),
            v((3, 256, 128), bf16),
            v((256, 128), f32),
            v((16, 128), bf16),
            v((4, 2048), bf16),
            v((16, 2048), bf16),
            v((2, 256), jnp.int32),
            v((4, 128), bf16),
            v((4, 256), bf16),
            v((4, 256), bf16),
            v((32, 128), f32),
            v((32, 128), f32),
            v((1, 128), bf16),
            dma((10,)),
            dma((8,)), dma((8,)), dma((8,)), dma((8,)),
            dma((16,)), dma((16,)), dma((16,)), dma((16,)),
            dma((4,)), dma((4,)), dma((2, 16)), dma((2, 16)),
            dma((8,)), dma((8,)), dma((2, 2, 4)), dma((2, 2, 4)), dma((8,)), dma((8,)),
            dma, dma, dma((3,)), dma((3,)), dma((16,)), dma((16,)),
            dma((3,)), dma((3,)),
        ],
        compiler_params=pltpu.CompilerParams(
            collective_id=0, has_side_effects=True, vmem_limit_bytes=56 * 1024 * 1024
        ),
    )(*args)


def per_device(
    mixer_input_channels,
    output_gate_logits,
    head_group_input_map,
    head_group_output_map,
    input_channel_taps,
    input_map_taps,
    output_map_taps,
    step_logits,
    head_log_rate,
    extra_log_decay,
    head_direct_scale,
    gated_norm_scale,
    mixer_output_weight,
    second_batch_tokens,
    pre_expert_norm_scale,
    group_router_columns,
    expert_router_columns,
    routes,
    expert_gate_weight,
    expert_up_weight,
    expert_down_weight,
):
    def by_block(v):
        return jnp.transpose(v.reshape(2, 16, 128), (1, 0, 2)).reshape(32, 128)

    return fused(
        pre_expert_norm_scale.reshape(16, 128),
        group_router_columns.T,
        expert_router_columns.T,
        routes.T,
        input_channel_taps,
        input_map_taps,
        output_map_taps,
        by_block(step_logits),
        by_block(extra_log_decay),
        gated_norm_scale.reshape(1, -1),
        head_log_rate,
        head_direct_scale,
        second_batch_tokens,
        expert_gate_weight[0],
        expert_up_weight[0],
        expert_down_weight[0],
        mixer_output_weight,
        mixer_input_channels,
        output_gate_logits,
        head_group_input_map,
        head_group_output_map,
    )


def solution(mesh):
    in_specs = (
        P("ep", "tp"),
        P("ep", "tp"),
        P("ep", None),
        P("ep", None),
        P(None, "tp"),
        P(),
        P(),
        P("tp", "ep"),
        P("tp"),
        P("tp", "ep"),
        P("tp"),
        P("tp"),
        P("tp", None),
        P("ep", None),
        P(),
        P(),
        P(),
        P("ep", None),
        P("ep", None, "tp"),
        P("ep", None, "tp"),
        P("ep", "tp", None),
    )
    out_specs = (P(("ep", "tp"), None), P("ep", "tp"))
    return jax.shard_map(
        per_device, mesh=mesh, in_specs=in_specs, out_specs=out_specs, check_vma=False
    )
```

```python
import jax
import jax.numpy as jnp
from jax import lax
from jax.experimental import pallas as pl
from jax.experimental.pallas import tpu as pltpu
from jax.sharding import PartitionSpec as P

eps = 1e-06
exact_prec = lax.Precision.HIGHEST
bf16, f32 = jnp.bfloat16, jnp.float32

NEP = 16
NZ = 8
CAP = 64
HALF = CAP // 2
ORDER = (4, 3, 5, 1, 2, 6, 7, 0)
NEAR = (
    (0, 0), (1, 0), (0, 1), (3, 0), (0, 3), (1, 1), (3, 3), (1, 3),
    (3, 1), (2, 0), (0, 2), (2, 1), (1, 2), (3, 2), (2, 3), (2, 2),
)
EARLY = 16


def kernel(
    nsc_h, rg_h, re_h, rt_h, ut_h, bt_h, ct_h, sl_h, ex_h, gn_h, rate, direct,
    tok_h, gate_h, up_h, down_h, w_h, u_h, og_h, bm_h, cm_h,
    mo, eo,
    nrm, sbuf, xr, gw, uw, dn, hall, ysend, ybuf, zsend, zbuf, wg, mx, psend, precv,
    ub, bb, cb, ogb, xsb, csb, c0l, c1l, dtl, cumr, dtr, tst, ssm, spad, ssend, sst, entb, mixb, keep_mine, tok, zway, zown,
    nsc, rg, re, rt, ut, bt, ct, sl, ex, gn, small_s, tok_s,
    loc_s, dnl_s, dns_s, dnr_s, xs_s, xr_s, xf_s, xg_s, hs_s, hr_s, ys_s, yr_s, zs_s, zr_s,
    ws_s, wr_s, ms_s, mr_s, fs_s, fr_s, hl_s, hh_s, ss_s, sr_s, zws_s, zwr_s,
):
    ep, tp = lax.axis_index("ep"), lax.axis_index("tp")
    y, x = ep // 4, ep % 4
    z, c = tp // 2, tp % 2
    other = z * 2 + (1 - c)

    def ep_at(d, sign):
        dx, dy = NEAR[d]
        return ((y + 4 + sign * dy) % 4) * 4 + (x + 4 + sign * dx) % 4

    def tp_at(r):
        return ((z + r) % NZ) * 2 + c

    def push(src, dst, ss, rs, e, t):
        return pltpu.make_async_remote_copy(
            src_ref=src, dst_ref=dst, send_sem=ss, recv_sem=rs,
            device_id={"ep": e, "tp": t}, device_id_type=pl.DeviceIdType.MESH,
        )

    barrier = pltpu.get_barrier_semaphore()

    def greet(e, t):
        pl.semaphore_signal(
            barrier, inc=1, device_id={"ep": e, "tp": t}, device_id_type=pl.DeviceIdType.MESH
        )

    lt = [
        pltpu.make_async_copy(tok_h.at[pl.ds(64 * i, 64), :], tok.at[pl.ds(64 * i, 64), :], tok_s.at[i])
        for i in range(4)
    ]
    for cp in lt:
        cp.start()
    for d in range(1, NEP):
        greet(ep_at(d, 1), tp)
    for r in range(1, NZ):
        greet(ep, tp_at(r))
    greet(ep, other)

    small = [
        pltpu.make_async_copy(src, dst, small_s.at[i])
        for i, (src, dst) in enumerate((
            (rt_h, rt), (nsc_h, nsc), (rg_h, rg), (re_h, re), (ut_h, ut), (bt_h, bt),
            (ct_h, ct), (sl_h, sl), (ex_h, ex), (gn_h, gn),
        ))
    ]
    for cp in small:
        cp.start()
    lg = pltpu.make_async_copy(gate_h, gw, loc_s.at[0])
    lu = pltpu.make_async_copy(up_h, uw, loc_s.at[1])
    lw = pltpu.make_async_copy(w_h, wg.at[pl.ds(0, 128), :], loc_s.at[2])
    grp = tp // 4
    map_cols = pl.ds(pl.multiple_of((grp // 2) * 128, 128), 128)
    body, tail = pl.ds(8, 2048), pl.ds(2040, 8)
    l_mix = [
        pltpu.make_async_copy(u_h, ub.at[body, :], loc_s.at[4]),
        pltpu.make_async_copy(bm_h.at[:, map_cols], bb.at[body, :], loc_s.at[5]),
        pltpu.make_async_copy(cm_h.at[:, map_cols], cb.at[body, :], loc_s.at[6]),
        pltpu.make_async_copy(og_h, ogb, loc_s.at[3]),
    ]
    for cp in l_mix + [lw]:
        cp.start()

    def down_cols(q, core):
        return down_h.at[:, pl.ds(pl.multiple_of((2 * ((z + ORDER[q]) % NZ) + core) * 128, 128), 128)]

    dn_l = [
        pltpu.make_async_copy(
            down_cols(q, c), dn.at[c, :, pl.ds(q * 128, 128)], dnl_s.at[q]
        )
        for q in range(NZ)
    ]

    for cp in small:
        cp.wait()
    norm_gain = jnp.concatenate([nsc[i : i + 1, :] for i in range(16)], axis=1).astype(f32)

    def norm_rows(i, _):
        rows = pl.ds(pl.multiple_of(i * 32, 32), 32)
        v = tok[rows, :].astype(f32)
        v = v * lax.rsqrt(jnp.mean(v * v, axis=1, keepdims=True) + eps) * norm_gain
        nrm[rows, :] = v.astype(bf16)
        return 0

    for i in range(4):
        lt[i].wait()
        lax.fori_loop(2 * i, 2 * i + 2, norm_rows, 0)

    r0, r1 = rt[0:1, :], rt[1:2, :]
    di = lax.broadcasted_iota(jnp.int32, (NEP, 256), 0)
    e_rel = jnp.zeros((NEP, 256), jnp.int32)
    for d in range(NEP):
        e_rel = jnp.where(di == d, ep_at(d, 1), e_rel)
    in0, in1 = e_rel == r0, e_rel == r1
    routed = in0 | in1
    onehot = jnp.where(routed, 1.0, 0.0).astype(bf16)
    a = lax.broadcasted_iota(jnp.int32, (256, 256), 0)
    b = lax.broadcasted_iota(jnp.int32, (256, 256), 1)
    before = jnp.where(a < b, 1.0, 0.0).astype(bf16)
    place = jnp.dot(onehot, before, preferred_element_type=f32)
    place = jnp.where(routed, place, -1.0)
    slot = lax.broadcasted_iota(jnp.int32, (HALF, 256), 0) + HALF * c
    slot = slot.astype(f32)
    tokens_n = nrm[...]
    for q in range(4):
        pick = jnp.concatenate(
            [jnp.where(place[d : d + 1, :] == slot, 1.0, 0.0) for d in range(4 * q, 4 * q + 4)], axis=0
        ).astype(bf16)
        sbuf[q * 128 : (q + 1) * 128, :] = jnp.dot(pick, tokens_n, preferred_element_type=f32).astype(bf16)
    pl.semaphore_wait(barrier, NEP - 1 + NZ - 1 + 1)
    after = (ep + 1) % NEP
    halo = [
        push(u_h.at[tail, :], ub.at[pl.ds(0, 8), :], hl_s.at[0], hh_s.at[0], after, tp),
        push(bm_h.at[tail, map_cols], bb.at[pl.ds(0, 8), :], hl_s.at[1], hh_s.at[1], after, tp),
        push(cm_h.at[tail, map_cols], cb.at[pl.ds(0, 8), :], hl_s.at[2], hh_s.at[2], after, tp),
    ]
    for cp in halo:
        cp.start()

    dn_r = [
        push(down_cols(q, 1 - c), dn.at[c, :, pl.ds(q * 128, 128)], dns_s.at[q], dnr_s.at[q], ep, other)
        for q in range(NZ)
    ]
    for cp in dn_r:
        cp.start()
    def w_copy(way, k, part):
        if way == 0:
            a, b, t = (9 - k) % NZ, NZ - k, tp_at(1)
        else:
            a, b, t = k - 1, k, tp_at(NZ - 1)
        lo = 64 * part
        src = w_h.at[pl.ds(lo, 64), :] if k == 1 else wg.at[pl.ds(a * 128 + lo, 64), :]
        return push(
            src, wg.at[pl.ds(b * 128 + lo, 64), :],
            ws_s.at[way, part, k - 1], wr_s.at[way, part, k - 1], ep, t,
        )

    w_cp = {
        (way, k, part): w_copy(way, k, part)
        for way in range(2) for k in range(1, 5) for part in range(2)
        if k < 4 or part == way
    }

    def w_step(k, part):
        for way in range(2):
            if (way, k, part) in w_cp:
                if k > 1:
                    w_cp[way, k - 1, part].wait_recv()
                w_cp[way, k, part].start()

    w_step(1, 0)
    w_step(1, 1)

    x_cp = [
        push(
            sbuf.at[pl.ds(d * HALF, HALF), :],
            xr.at[pl.ds(pl.multiple_of(d * CAP + HALF * c, HALF), HALF), :],
            xs_s.at[d], xr_s.at[d], ep_at(d, 1), tp,
        )
        for d in range(1, NEP)
    ]
    for cp in x_cp[:EARLY]:
        cp.start()
    for cp in dn_l + [lg, lu]:
        cp.start()
    xr[pl.ds(pl.multiple_of(HALF * c, HALF), HALF), :] = sbuf[0:HALF, :]

    def x_hand(d):
        rows = pl.ds(pl.multiple_of(d * CAP + HALF * c, HALF), HALF)
        return push(xr.at[rows, :], xr.at[rows, :], xf_s.at[d], xg_s.at[d], ep, other)

    hand = [x_hand(d) for d in range(NEP)]

    def pass_on(g):
        for d in range(4 * g, 4 * g + 4):
            if d > 0:
                x_cp[d - 1].wait_recv()
            hand[d].start()

    nt = (((1,), (1,)), ((), ()))
    gl = lax.dot_general(rg[...], tokens_n, nt, preferred_element_type=f32)
    el = lax.dot_general(re[...], tokens_n, nt, preferred_element_type=f32)

    def lse(v):
        top = jnp.max(v, axis=0, keepdims=True)
        return top + jnp.log(jnp.sum(jnp.exp(v - top), axis=0, keepdims=True))

    gl = gl - lse(gl)
    ei = lax.broadcasted_iota(jnp.int32, (4, 256), 0)
    lp0 = jnp.zeros((1, 256), f32)
    lp1 = jnp.zeros((1, 256), f32)
    for g in range(4):
        part = el[4 * g : 4 * g + 4, :]
        part = part - lse(part) + gl[g : g + 1, :]
        lp0 += jnp.sum(jnp.where(ei + 4 * g == r0, part, 0.0), axis=0, keepdims=True)
        lp1 += jnp.sum(jnp.where(ei + 4 * g == r1, part, 0.0), axis=0, keepdims=True)
    top = jnp.maximum(lp0, lp1)
    w0, w1 = jnp.exp(lp0 - top), jnp.exp(lp1 - top)
    total = w0 + w1
    share = jnp.where(in0, w0 / total, 0.0) + jnp.where(in1, w1 / total, 0.0)
    both = jnp.concatenate([place, share, jnp.zeros((96, 256), f32)], axis=0).T

    lane = lax.broadcasted_iota(jnp.int32, (256, 128), 1)
    in_slot = (lane & (CAP - 1)).astype(f32)
    low = lane < CAP
    mixw = []
    for p in range(8):
        at = jnp.where(low, both[:, 2 * p : 2 * p + 1], both[:, 2 * p + 1 : 2 * p + 2])
        sh = jnp.where(low, both[:, 16 + 2 * p : 17 + 2 * p], both[:, 17 + 2 * p : 18 + 2 * p])
        mixw.append(jnp.where(at == in_slot, sh, 0.0).astype(bf16))
    mixw = jnp.concatenate(mixw, axis=1)

    row = lax.broadcasted_iota(jnp.int32, (32, 128), 0)
    lane1 = lax.broadcasted_iota(jnp.int32, (1, 128), 1)
    first = lax.broadcasted_iota(jnp.int32, (128, 128), 1) < 64
    at_l = lax.broadcasted_iota(jnp.int32, (128, 128), 0)
    at_s = lax.broadcasted_iota(jnp.int32, (128, 128), 1)
    lower = at_l >= at_s
    sv = sl[...]
    dt = jnp.maximum(sv, 0.0) + jnp.log1p(jnp.exp(-jnp.abs(sv)))
    speed = jnp.exp(jnp.where((row & 1) == 0, rate[0], rate[1]))
    log_decay = ex[...] - dt * speed
    upto = jnp.where(at_l <= at_s, 1.0, 0.0).astype(f32)
    cum = jnp.dot(log_decay, upto, precision=exact_prec, preferred_element_type=f32)
    cumr[...] = cum
    dtr[...] = dt
    turned = jnp.concatenate([cum, dt, jnp.zeros((64, 128), f32)], axis=0).T
    for b in range(16):
        rows = slice(128 * b, 128 * (b + 1))
        c0l[rows, :] = jnp.broadcast_to(turned[:, 2 * b : 2 * b + 1], (128, 128))
        c1l[rows, :] = jnp.broadcast_to(turned[:, 2 * b + 1 : 2 * b + 2], (128, 128))
        dtl[rows, :] = jnp.where(first, turned[:, 32 + 2 * b : 33 + 2 * b], turned[:, 33 + 2 * b : 34 + 2 * b])

    for cp in l_mix:
        cp.wait()
    for cp in halo:
        cp.wait_recv()
    for buf in (ub, bb, cb):
        edge = buf[0:8, :]
        buf[0:8, :] = jnp.where(ep == 0, jnp.zeros_like(edge), edge)
    tap_u = ut[...].astype(f32)
    block_0 = grp // 2 == 0
    tap_b = jnp.where(block_0, bt[:, 0:128].astype(f32), bt[:, 128:256].astype(f32))
    tap_c = jnp.where(block_0, ct[:, 0:128].astype(f32), ct[:, 128:256].astype(f32))
    own_half = (lane1 // 64) == grp % 2

    def conv(buf, taps, base):
        ext = buf[pl.ds(base, 136), :].astype(f32)
        tot = taps[0:1, :] * ext[5:133, :]
        for j in range(1, 4):
            tot += taps[j : j + 1, :] * ext[5 + j : 133 + j, :]
        return tot * jax.nn.sigmoid(tot)

    def one_block(b, carry):
        state, since = carry
        base = pl.multiple_of(b * 128, 128)
        rows = pl.ds(base, 128)
        xs = conv(ub, tap_u, base).astype(bf16)
        bs = conv(bb, tap_b, base).astype(bf16)
        cs = jnp.where(own_half, conv(cb, tap_c, base), 0.0).astype(bf16)
        xsb[rows, :] = xs
        csb[rows, :] = cs
        tst[pl.ds(b, 1), :] = since
        scores = lax.dot_general(cs, bs, (((1,), (1,)), ((), ())), preferred_element_type=f32)
        inner = []
        for h, col in ((0, c0l), (1, c1l)):
            at = pl.ds(2 * b + h, 1)
            diff = jnp.where(lower, col[rows, :] - cumr[at, :], 0.0)
            near = jnp.where(lower, scores * jnp.exp(diff) * dtr[at, :], 0.0).astype(bf16)
            inner.append(jnp.dot(near, xs, preferred_element_type=f32))
        both_cum = jnp.where(first, c0l[rows, :], c1l[rows, :])
        carried = jnp.dot(cs, state.astype(bf16), preferred_element_type=f32) * jnp.exp(both_cum)
        ssm[rows, :] = jnp.where(first, inner[0], inner[1]) + carried
        last = both_cum[127:128, :]
        weighed = (xs.astype(f32) * (jnp.exp(last - both_cum) * dtl[rows, :])).astype(bf16)
        gained = lax.dot_general(bs, weighed, (((0,), (0,)), ((), ())), preferred_element_type=f32)
        return state * jnp.exp(last) + gained, since + last

    carry = lax.fori_loop(
        0, 8, one_block, (jnp.zeros((128, 128), f32), jnp.zeros((1, 128), f32))
    )
    w_step(2, 0)
    state, since = lax.fori_loop(8, 16, one_block, carry)
    spad[...] = state
    half_rows = pl.ds(pl.multiple_of((grp % 2) * 64, 64), 64)
    ssend[0:64, :] = spad[half_rows, :].astype(bf16)
    decay = jnp.exp(since)
    near_decay = decay.astype(bf16)
    rest_decay = (decay - near_decay.astype(f32)).astype(bf16)
    row8 = lax.broadcasted_iota(jnp.int32, (8, 128), 0)
    ssend[64:72, :] = jnp.where(
        row8 == 0, near_decay.astype(f32), jnp.where(row8 == 1, rest_decay.astype(f32), 0.0)
    ).astype(bf16)
    s_cp = [
        push(ssend, sst.at[ep], ss_s.at[d], sr_s.at[d], ep_at(d, 1), tp) for d in range(1, NEP)
    ]
    for cp in s_cp:
        cp.start()
    for cp in x_cp[EARLY:]:
        cp.start()
    w_step(2, 1)


    def mixer_rest():
        for cp in s_cp:
            cp.wait_recv()

        def chain(j, ent):
            got = sst[j].astype(f32)
            return jnp.where(j < ep, ent * (got[64:65, :] + got[65:66, :]) + got[0:64, :], ent)

        ent = lax.fori_loop(0, NEP - 1, chain, jnp.zeros((64, 128), f32))
        entb[...] = jnp.zeros_like(entb)
        entb[half_rows, :] = ent.astype(bf16)
        scale = jnp.where(lane1 < 64, direct[0], direct[1])
        gain = gn[...].astype(f32)

        def rows_of(j, keep):
            for k in range(2):
                b = 2 * j + k
                rows = pl.ds(pl.multiple_of(b * 128, 128), 128)
                since_b = jnp.where(first, c0l[rows, :], c1l[rows, :]) + tst[pl.ds(b, 1), :]
                far = jnp.dot(csb[rows, :], entb[...], preferred_element_type=f32) * jnp.exp(since_b)
                gate = ogb[rows, :].astype(f32)
                val = (ssm[rows, :] + far + scale * xsb[rows, :].astype(f32)) * (gate * jax.nn.sigmoid(gate))
                sq = val * val
                sum0 = jnp.sum(jnp.where(first, sq, 0.0), axis=1, keepdims=True)
                sum1 = jnp.sum(jnp.where(first, 0.0, sq), axis=1, keepdims=True)
                ms = jnp.where(first, sum0, sum1) * (1.0 / 64)
                keep(k, rows, (val * lax.rsqrt(ms + eps) * gain).astype(bf16))

        def send_on(i, _):
            j = (z + 1 + i) % NZ

            def keep(k, rows, val):
                mixb[rows, :] = val

            rows_of(j, keep)
            push(
                mixb.at[pl.ds(pl.multiple_of(j * 256, 256), 256), :],
                mx.at[:, pl.ds(pl.multiple_of((7 - i) * 128, 128), 128)],
                ms_s.at[7 - i], mr_s.at[7 - i], ep, tp_at(1 + i),
            ).start()
            return 0

        lax.fori_loop(0, NZ - 1, send_on, 0)

        def own(k, rows, val):
            mx[128 * k : 128 * (k + 1), 0:128] = val

        rows_of(z, own)

    m_cp = [
        push(
            mixb.at[pl.ds(pl.multiple_of(((z + r) % NZ) * 256, 256), 256), :],
            mx.at[:, pl.ds((NZ - r) * 128, 128)],
            ms_s.at[NZ - r], mr_s.at[NZ - r], ep, tp_at(r),
        )
        for r in range(1, NZ)
    ]

    lg.wait()
    lu.wait()
    for cp in dn_l:
        cp.wait()

    def y_copy(d, h):
        part = (pl.ds(d * CAP, CAP), pl.ds(h * 512, 512))
        return push(ysend.at[part], ybuf.at[part], ys_s.at[h, d], yr_s.at[h, d], ep_at(d, -1), tp)

    y_cp = [[y_copy(d, h) for d in range(1, NEP)] for h in range(2)]
    h_cp = []
    for g in range(4):
        part = hall.at[c, pl.ds(256 * g, 256), :]
        h_cp.append(push(part, part, hs_s.at[g], hr_s.at[g], ep, other))

    def hidden(g):
        for d in range(4 * g, 4 * g + 4):
            hand[d].wait_recv()
        rows = slice(256 * g, 256 * (g + 1))
        xg = xr[rows, :]
        gv = jnp.dot(xg, gw[...], preferred_element_type=f32)
        uv = jnp.dot(xg, uw[...], preferred_element_type=f32)
        hall[c, rows, :] = (gv * jax.nn.sigmoid(gv) * uv).astype(bf16)
        h_cp[g].start()

    def results(g):
        rows = slice(256 * g, 256 * (g + 1))
        h_cp[g].wait_recv()
        yv = jnp.dot(hall[0, rows, :], dn[0], preferred_element_type=f32)
        yv += jnp.dot(hall[1, rows, :], dn[1], preferred_element_type=f32)
        ysend[rows, :] = yv.astype(bf16)
        for d in range(4 * g, 4 * g + 4):
            if d > 0:
                y_cp[0][d - 1].start()

    pass_on(0)
    pass_on(1)
    hidden(0)
    hidden(1)
    for cq in dn_r:
        cq.wait_recv()
    w_step(3, 0)
    results(0)
    results(1)
    w_step(3, 1)
    pass_on(2)
    hidden(2)
    pass_on(3)
    results(2)
    hidden(3)
    results(3)
    for d in range(1, NEP):
        y_cp[1][d - 1].start()
    w_step(4, 0)
    w_step(4, 1)
    mixer_rest()
    ybuf[0:CAP, :] = ysend[0:CAP, :]

    def project():
        lw.wait()
        for cp in m_cp:
            cp.wait_recv()
        for way in range(2):
            w_cp[way, 3, 1 - way].wait_recv()
            w_cp[way, 4, way].wait_recv()
        theirs = mx[pl.ds(pl.multiple_of((1 - c) * 128, 128), 128), :]
        psend[...] = jnp.dot(theirs, wg[...], preferred_element_type=f32).astype(bf16)
        fin = push(psend, precv, fs_s, fr_s, ep, other)
        fin.start()
        ours = mx[pl.ds(pl.multiple_of(c * 128, 128), 128), :]
        mine = jnp.dot(ours, wg[...], preferred_element_type=f32)
        keep_mine[...] = mine
        return fin

    first_hop = {4: (2, 0), 3: (1, 1), 5: (7, 2)}
    z_cp, on_way = [], []
    for h in range(2):
        for d in range(1, NEP):
            y_cp[h][d - 1].wait_recv()
        cols = slice(512 * h, 512 * (h + 1))
        comb = jnp.dot(mixw, ybuf[:, cols], preferred_element_type=f32)
        for i in ((0, 1, 2, 3), (2, 3, 0, 1))[h]:
            r = ORDER[4 * h + i]
            if r == 2:
                for cp in on_way:
                    cp.wait_recv()
            val = comb[:, 128 * i : 128 * (i + 1)]
            if r == 0:
                zown[...] = val
                continue
            if r in first_hop:
                hop, place_w = first_hop[r]
                zsend[r] = val.astype(bf16)
                cp = push(zsend.at[r], zway.at[place_w], zws_s.at[place_w], zwr_s.at[place_w], ep, tp_at(hop))
                cp.start()
                on_way.append(cp)
                continue
            if r == 2:
                val = val + zway[0].astype(f32) + zway[1].astype(f32)
            if r == 6:
                val = val + zway[2].astype(f32)
            zsend[r] = val.astype(bf16)
            cp = push(zsend.at[r], zbuf.at[NZ - r], zs_s.at[NZ - r], zr_s.at[NZ - r], ep, tp_at(r))
            cp.start()
            z_cp.append(cp)

    fin = project()
    fin.wait_recv()
    mo[...] = (keep_mine[...] + precv[...].astype(f32)).astype(bf16)

    acc = zown[...]
    for cp in z_cp:
        cp.wait_recv()
    for r in (1, 2, 6, 7):
        acc += zbuf[r].astype(f32)
    eo[...] = acc.astype(bf16)

    for cp in dn_r + m_cp + x_cp + halo + s_cp + hand + y_cp[0] + y_cp[1] + h_cp + z_cp + on_way + [fin]:
        cp.wait_send()
    for cp in w_cp.values():
        cp.wait_send()


def fused(*args):
    vmem, hbm = pl.BlockSpec(memory_space=pltpu.VMEM), pl.BlockSpec(memory_space=pl.ANY)
    smem = pl.BlockSpec(memory_space=pltpu.SMEM)
    dma = pltpu.SemaphoreType.DMA
    v = pltpu.VMEM
    return pl.pallas_call(
        kernel,
        out_shape=(
            pltpu.VMEM((128, 2048), bf16),
            pltpu.VMEM((256, 128), bf16),
        ),
        in_specs=[hbm] * 10 + [smem] * 2 + [hbm] * 9,
        out_specs=(vmem, vmem),
        scratch_shapes=[
            v((256, 2048), bf16),
            v((512, 2048), bf16),
            v((1024, 2048), bf16),
            v((2048, 256), bf16),
            v((2048, 256), bf16),
            v((2, 256, 1024), bf16),
            v((2, 1024, 256), bf16),
            v((1024, 1024), bf16),
            v((1024, 1024), bf16),
            v((8, 256, 128), bf16),
            v((8, 256, 128), bf16),
            v((1024, 2048), bf16),
            v((256, 1024), bf16),
            v((128, 2048), bf16),
            v((128, 2048), bf16),
            v((2056, 128), bf16),
            v((2056, 128), bf16),
            v((2056, 128), bf16),
            v((2048, 128), bf16),
            v((2048, 128), bf16),
            v((2048, 128), bf16),
            v((2048, 128), f32),
            v((2048, 128), f32),
            v((2048, 128), f32),
            v((32, 128), f32),
            v((32, 128), f32),
            v((16, 128), f32),
            v((2048, 128), f32),
            v((128, 128), f32),
            v((72, 128), bf16),
            v((16, 72, 128), bf16),
            v((128, 128), bf16),
            v((2048, 128), bf16),
            v((128, 2048), f32),
            v((256, 2048), bf16),
            v((3, 256, 128), bf16),
            v((256, 128), f32),
            v((16, 128), bf16),
            v((4, 2048), bf16),
            v((16, 2048), bf16),
            v((2, 256), jnp.int32),
            v((4, 128), bf16),
            v((4, 256), bf16),
            v((4, 256), bf16),
            v((32, 128), f32),
            v((32, 128), f32),
            v((1, 128), bf16),
            dma((10,)),
            dma((4,)),
            dma((8,)), dma((8,)), dma((8,)), dma((8,)),
            dma((16,)), dma((16,)), dma((16,)), dma((16,)),
            dma((4,)), dma((4,)), dma((2, 16)), dma((2, 16)),
            dma((8,)), dma((8,)), dma((2, 2, 4)), dma((2, 2, 4)), dma((8,)), dma((8,)),
            dma, dma, dma((3,)), dma((3,)), dma((16,)), dma((16,)),
            dma((3,)), dma((3,)),
        ],
        compiler_params=pltpu.CompilerParams(
            collective_id=0, has_side_effects=True, vmem_limit_bytes=56 * 1024 * 1024
        ),
    )(*args)


def per_device(
    mixer_input_channels,
    output_gate_logits,
    head_group_input_map,
    head_group_output_map,
    input_channel_taps,
    input_map_taps,
    output_map_taps,
    step_logits,
    head_log_rate,
    extra_log_decay,
    head_direct_scale,
    gated_norm_scale,
    mixer_output_weight,
    second_batch_tokens,
    pre_expert_norm_scale,
    group_router_columns,
    expert_router_columns,
    routes,
    expert_gate_weight,
    expert_up_weight,
    expert_down_weight,
):
    def by_block(v):
        return jnp.transpose(v.reshape(2, 16, 128), (1, 0, 2)).reshape(32, 128)

    return fused(
        pre_expert_norm_scale.reshape(16, 128),
        group_router_columns.T,
        expert_router_columns.T,
        routes.T,
        input_channel_taps,
        input_map_taps,
        output_map_taps,
        by_block(step_logits),
        by_block(extra_log_decay),
        gated_norm_scale.reshape(1, -1),
        head_log_rate,
        head_direct_scale,
        second_batch_tokens,
        expert_gate_weight[0],
        expert_up_weight[0],
        expert_down_weight[0],
        mixer_output_weight,
        mixer_input_channels,
        output_gate_logits,
        head_group_input_map,
        head_group_output_map,
    )


def solution(mesh):
    in_specs = (
        P("ep", "tp"),
        P("ep", "tp"),
        P("ep", None),
        P("ep", None),
        P(None, "tp"),
        P(),
        P(),
        P("tp", "ep"),
        P("tp"),
        P("tp", "ep"),
        P("tp"),
        P("tp"),
        P("tp", None),
        P("ep", None),
        P(),
        P(),
        P(),
        P("ep", None),
        P("ep", None, "tp"),
        P("ep", None, "tp"),
        P("ep", "tp", None),
    )
    out_specs = (P(("ep", "tp"), None), P("ep", "tp"))
    return jax.shard_map(
        per_device, mesh=mesh, in_specs=in_specs, out_specs=out_specs, check_vma=False
    )
```

```python
import jax
import jax.numpy as jnp
from jax import lax
from jax.experimental import pallas as pl
from jax.experimental.pallas import tpu as pltpu
from jax.sharding import PartitionSpec as P

eps = 1e-06
exact_prec = lax.Precision.HIGHEST
bf16, f32 = jnp.bfloat16, jnp.float32

NEP = 16
NZ = 8
CAP = 64
HALF = CAP // 2
ORDER = (4, 3, 5, 1, 2, 6, 7, 0)
NEAR = (
    (0, 0), (1, 0), (0, 1), (3, 0), (0, 3), (1, 1), (3, 3), (1, 3),
    (3, 1), (2, 0), (0, 2), (2, 1), (1, 2), (3, 2), (2, 3), (2, 2),
)


def kernel(
    nsc_h, rg_h, re_h, rt_h, ut_h, bt_h, ct_h, sl_h, ex_h, gn_h, rate, direct,
    tok_h, gate_h, up_h, down_h, w_h, u_h, og_h, bm_h, cm_h,
    mo, eo,
    nrm, sbuf, xr, gw, uw, dn, hall, ysend, ybuf, zsend, zbuf, wg, mx, psend, precv,
    ub, bb, cb, ogb, xsb, csb, c0l, c1l, dtl, cumr, dtr, tst, ssm, spad, ssend, sst, entb, mixb, keep_mine, tok, zway, zown,
    nsc, rg, re, rt, ut, bt, ct, sl, ex, gn, small_s, tok_s,
    loc_s, dnl_s, dns_s, dnr_s, xs_s, xr_s, xf_s, xg_s, hs_s, hr_s, ys_s, yr_s, zs_s, zr_s,
    ws_s, wr_s, ms_s, mr_s, fs_s, fr_s, hl_s, hh_s, ss_s, sr_s, zws_s, zwr_s,
):
    ep, tp = lax.axis_index("ep"), lax.axis_index("tp")
    y, x = ep // 4, ep % 4
    z, c = tp // 2, tp % 2
    other = z * 2 + (1 - c)

    def ep_at(d, sign):
        dx, dy = NEAR[d]
        return ((y + 4 + sign * dy) % 4) * 4 + (x + 4 + sign * dx) % 4

    def tp_at(r):
        return ((z + r) % NZ) * 2 + c

    def push(src, dst, ss, rs, e, t):
        return pltpu.make_async_remote_copy(
            src_ref=src, dst_ref=dst, send_sem=ss, recv_sem=rs,
            device_id={"ep": e, "tp": t}, device_id_type=pl.DeviceIdType.MESH,
        )

    barrier = pltpu.get_barrier_semaphore()

    def greet(e, t):
        pl.semaphore_signal(
            barrier, inc=1, device_id={"ep": e, "tp": t}, device_id_type=pl.DeviceIdType.MESH
        )

    lt = [
        pltpu.make_async_copy(tok_h.at[pl.ds(64 * i, 64), :], tok.at[pl.ds(64 * i, 64), :], tok_s.at[i])
        for i in range(4)
    ]
    for cp in lt:
        cp.start()
    for d in range(1, NEP):
        greet(ep_at(d, 1), tp)
    for r in range(1, NZ):
        greet(ep, tp_at(r))
    greet(ep, other)

    small = [
        pltpu.make_async_copy(src, dst, small_s.at[i])
        for i, (src, dst) in enumerate((
            (rt_h, rt), (nsc_h, nsc), (rg_h, rg), (re_h, re), (ut_h, ut), (bt_h, bt),
            (ct_h, ct), (sl_h, sl), (ex_h, ex), (gn_h, gn),
        ))
    ]
    for cp in small:
        cp.start()
    lg = pltpu.make_async_copy(gate_h, gw, loc_s.at[0])
    lu = pltpu.make_async_copy(up_h, uw, loc_s.at[1])
    lw = pltpu.make_async_copy(w_h, wg.at[pl.ds(0, 128), :], loc_s.at[2])
    grp = tp // 4
    map_cols = pl.ds(pl.multiple_of((grp // 2) * 128, 128), 128)
    body, tail = pl.ds(8, 2048), pl.ds(2040, 8)
    l_mix = [
        pltpu.make_async_copy(u_h, ub.at[body, :], loc_s.at[4]),
        pltpu.make_async_copy(bm_h.at[:, map_cols], bb.at[body, :], loc_s.at[5]),
        pltpu.make_async_copy(cm_h.at[:, map_cols], cb.at[body, :], loc_s.at[6]),
        pltpu.make_async_copy(og_h, ogb, loc_s.at[3]),
    ]
    for cp in l_mix + [lw]:
        cp.start()

    def down_cols(q, core):
        return down_h.at[:, pl.ds(pl.multiple_of((2 * ((z + ORDER[q]) % NZ) + core) * 128, 128), 128)]

    dn_l = [
        pltpu.make_async_copy(
            down_cols(q, c), dn.at[c, :, pl.ds(q * 128, 128)], dnl_s.at[q]
        )
        for q in range(NZ)
    ]

    for cp in small:
        cp.wait()
    norm_gain = jnp.concatenate([nsc[i : i + 1, :] for i in range(16)], axis=1).astype(f32)

    def norm_rows(i, _):
        rows = pl.ds(pl.multiple_of(i * 16, 16), 16)
        v = tok[rows, :].astype(f32)
        v = v * lax.rsqrt(jnp.mean(v * v, axis=1, keepdims=True) + eps) * norm_gain
        nrm[rows, :] = v.astype(bf16)
        return 0

    for i in range(4):
        lt[i].wait()
        lax.fori_loop(4 * i, 4 * i + 4, norm_rows, 0)

    r0, r1 = rt[0:1, :], rt[1:2, :]
    di = lax.broadcasted_iota(jnp.int32, (NEP, 256), 0)
    e_rel = jnp.zeros((NEP, 256), jnp.int32)
    for d in range(NEP):
        e_rel = jnp.where(di == d, ep_at(d, 1), e_rel)
    in0, in1 = e_rel == r0, e_rel == r1
    routed = in0 | in1
    onehot = jnp.where(routed, 1.0, 0.0).astype(bf16)
    a = lax.broadcasted_iota(jnp.int32, (256, 256), 0)
    b = lax.broadcasted_iota(jnp.int32, (256, 256), 1)
    before = jnp.where(a < b, 1.0, 0.0).astype(bf16)
    place = jnp.dot(onehot, before, preferred_element_type=f32)
    place = jnp.where(routed, place, -1.0)
    slot = lax.broadcasted_iota(jnp.int32, (HALF, 256), 0) + HALF * c
    slot = slot.astype(f32)
    pl.semaphore_wait(barrier, NEP - 1 + NZ - 1 + 1)
    after = (ep + 1) % NEP
    halo = [
        push(u_h.at[tail, :], ub.at[pl.ds(0, 8), :], hl_s.at[0], hh_s.at[0], after, tp),
        push(bm_h.at[tail, map_cols], bb.at[pl.ds(0, 8), :], hl_s.at[1], hh_s.at[1], after, tp),
        push(cm_h.at[tail, map_cols], cb.at[pl.ds(0, 8), :], hl_s.at[2], hh_s.at[2], after, tp),
    ]
    for cp in halo:
        cp.start()

    dn_r = [
        push(down_cols(q, 1 - c), dn.at[c, :, pl.ds(q * 128, 128)], dns_s.at[q], dnr_s.at[q], ep, other)
        for q in range(NZ)
    ]
    def w_copy(way, k, part):
        if way == 0:
            a, b, t = (9 - k) % NZ, NZ - k, tp_at(1)
        else:
            a, b, t = k - 1, k, tp_at(NZ - 1)
        lo = 64 * part
        src = w_h.at[pl.ds(lo, 64), :] if k == 1 else wg.at[pl.ds(a * 128 + lo, 64), :]
        return push(
            src, wg.at[pl.ds(b * 128 + lo, 64), :],
            ws_s.at[way, part, k - 1], wr_s.at[way, part, k - 1], ep, t,
        )

    w_cp = {
        (way, k, part): w_copy(way, k, part)
        for way in range(2) for k in range(1, 5) for part in range(2)
        if k < 4 or part == way
    }

    def w_step(k, part):
        for way in range(2):
            if (way, k, part) in w_cp:
                if k > 1:
                    w_cp[way, k - 1, part].wait_recv()
                w_cp[way, k, part].start()

    w_step(1, 0)
    w_step(1, 1)

    x_cp = [
        push(
            sbuf.at[pl.ds(d * HALF, HALF), :],
            xr.at[pl.ds(pl.multiple_of(d * CAP + HALF * c, HALF), HALF), :],
            xs_s.at[d], xr_s.at[d], ep_at(d, 1), tp,
        )
        for d in range(1, NEP)
    ]
    tokens_n = nrm[...]
    for q in range(4):
        pick = jnp.concatenate(
            [jnp.where(place[d : d + 1, :] == slot, 1.0, 0.0) for d in range(4 * q, 4 * q + 4)], axis=0
        ).astype(bf16)
        sbuf[q * 128 : (q + 1) * 128, :] = jnp.dot(pick, tokens_n, preferred_element_type=f32).astype(bf16)
        for d in range(max(1, 4 * q), 4 * q + 4):
            x_cp[d - 1].start()
    for cp in dn_r + dn_l + [lg, lu]:
        cp.start()
    xr[pl.ds(pl.multiple_of(HALF * c, HALF), HALF), :] = sbuf[0:HALF, :]

    def x_hand(d):
        rows = pl.ds(pl.multiple_of(d * CAP + HALF * c, HALF), HALF)
        return push(xr.at[rows, :], xr.at[rows, :], xf_s.at[d], xg_s.at[d], ep, other)

    hand = [x_hand(d) for d in range(NEP)]

    def pass_on(g):
        for d in range(4 * g, 4 * g + 4):
            if d > 0:
                x_cp[d - 1].wait_recv()
            hand[d].start()

    nt = (((1,), (1,)), ((), ()))
    gl = lax.dot_general(rg[...], tokens_n, nt, preferred_element_type=f32)
    el = lax.dot_general(re[...], tokens_n, nt, preferred_element_type=f32)

    def lse(v):
        top = jnp.max(v, axis=0, keepdims=True)
        return top + jnp.log(jnp.sum(jnp.exp(v - top), axis=0, keepdims=True))

    gl = gl - lse(gl)
    ei = lax.broadcasted_iota(jnp.int32, (4, 256), 0)
    lp0 = jnp.zeros((1, 256), f32)
    lp1 = jnp.zeros((1, 256), f32)
    for g in range(4):
        part = el[4 * g : 4 * g + 4, :]
        part = part - lse(part) + gl[g : g + 1, :]
        lp0 += jnp.sum(jnp.where(ei + 4 * g == r0, part, 0.0), axis=0, keepdims=True)
        lp1 += jnp.sum(jnp.where(ei + 4 * g == r1, part, 0.0), axis=0, keepdims=True)
    top = jnp.maximum(lp0, lp1)
    w0, w1 = jnp.exp(lp0 - top), jnp.exp(lp1 - top)
    total = w0 + w1
    share = jnp.where(in0, w0 / total, 0.0) + jnp.where(in1, w1 / total, 0.0)
    both = jnp.concatenate([place, share, jnp.zeros((96, 256), f32)], axis=0).T

    lane = lax.broadcasted_iota(jnp.int32, (256, 128), 1)
    in_slot = (lane & (CAP - 1)).astype(f32)
    low = lane < CAP
    mixw = []
    for p in range(8):
        at = jnp.where(low, both[:, 2 * p : 2 * p + 1], both[:, 2 * p + 1 : 2 * p + 2])
        sh = jnp.where(low, both[:, 16 + 2 * p : 17 + 2 * p], both[:, 17 + 2 * p : 18 + 2 * p])
        mixw.append(jnp.where(at == in_slot, sh, 0.0).astype(bf16))
    mixw = jnp.concatenate(mixw, axis=1)

    row = lax.broadcasted_iota(jnp.int32, (32, 128), 0)
    lane1 = lax.broadcasted_iota(jnp.int32, (1, 128), 1)
    first = lax.broadcasted_iota(jnp.int32, (128, 128), 1) < 64
    at_l = lax.broadcasted_iota(jnp.int32, (128, 128), 0)
    at_s = lax.broadcasted_iota(jnp.int32, (128, 128), 1)
    lower = at_l >= at_s
    sv = sl[...]
    dt = jnp.maximum(sv, 0.0) + jnp.log1p(jnp.exp(-jnp.abs(sv)))
    speed = jnp.exp(jnp.where((row & 1) == 0, rate[0], rate[1]))
    log_decay = ex[...] - dt * speed
    upto = jnp.where(at_l <= at_s, 1.0, 0.0).astype(f32)
    cum = jnp.dot(log_decay, upto, precision=exact_prec, preferred_element_type=f32)
    cumr[...] = cum
    dtr[...] = dt
    turned = jnp.concatenate([cum, dt, jnp.zeros((64, 128), f32)], axis=0).T
    for b in range(16):
        rows = slice(128 * b, 128 * (b + 1))
        c0l[rows, :] = jnp.broadcast_to(turned[:, 2 * b : 2 * b + 1], (128, 128))
        c1l[rows, :] = jnp.broadcast_to(turned[:, 2 * b + 1 : 2 * b + 2], (128, 128))
        dtl[rows, :] = jnp.where(first, turned[:, 32 + 2 * b : 33 + 2 * b], turned[:, 33 + 2 * b : 34 + 2 * b])

    for cp in l_mix:
        cp.wait()
    for cp in halo:
        cp.wait_recv()
    for buf in (ub, bb, cb):
        edge = buf[0:8, :]
        buf[0:8, :] = jnp.where(ep == 0, jnp.zeros_like(edge), edge)
    tap_u = ut[...].astype(f32)
    block_0 = grp // 2 == 0
    tap_b = jnp.where(block_0, bt[:, 0:128].astype(f32), bt[:, 128:256].astype(f32))
    tap_c = jnp.where(block_0, ct[:, 0:128].astype(f32), ct[:, 128:256].astype(f32))
    own_half = (lane1 // 64) == grp % 2

    def conv(buf, taps, base):
        ext = buf[pl.ds(base, 136), :].astype(f32)
        tot = taps[0:1, :] * ext[5:133, :]
        for j in range(1, 4):
            tot += taps[j : j + 1, :] * ext[5 + j : 133 + j, :]
        return tot * jax.nn.sigmoid(tot)

    def one_block(b, carry):
        state, since = carry
        base = pl.multiple_of(b * 128, 128)
        rows = pl.ds(base, 128)
        xs = conv(ub, tap_u, base).astype(bf16)
        bs = conv(bb, tap_b, base).astype(bf16)
        cs = jnp.where(own_half, conv(cb, tap_c, base), 0.0).astype(bf16)
        xsb[rows, :] = xs
        csb[rows, :] = cs
        tst[pl.ds(b, 1), :] = since
        scores = lax.dot_general(cs, bs, (((1,), (1,)), ((), ())), preferred_element_type=f32)
        inner = []
        for h, col in ((0, c0l), (1, c1l)):
            at = pl.ds(2 * b + h, 1)
            diff = jnp.where(lower, col[rows, :] - cumr[at, :], 0.0)
            near = jnp.where(lower, scores * jnp.exp(diff) * dtr[at, :], 0.0).astype(bf16)
            inner.append(jnp.dot(near, xs, preferred_element_type=f32))
        both_cum = jnp.where(first, c0l[rows, :], c1l[rows, :])
        carried = jnp.dot(cs, state.astype(bf16), preferred_element_type=f32) * jnp.exp(both_cum)
        ssm[rows, :] = jnp.where(first, inner[0], inner[1]) + carried
        last = both_cum[127:128, :]
        weighed = (xs.astype(f32) * (jnp.exp(last - both_cum) * dtl[rows, :])).astype(bf16)
        gained = lax.dot_general(bs, weighed, (((0,), (0,)), ((), ())), preferred_element_type=f32)
        return state * jnp.exp(last) + gained, since + last

    carry = lax.fori_loop(
        0, 8, one_block, (jnp.zeros((128, 128), f32), jnp.zeros((1, 128), f32))
    )
    w_step(2, 0)
    state, since = lax.fori_loop(8, 16, one_block, carry)
    spad[...] = state
    half_rows = pl.ds(pl.multiple_of((grp % 2) * 64, 64), 64)
    ssend[0:64, :] = spad[half_rows, :].astype(bf16)
    decay = jnp.exp(since)
    near_decay = decay.astype(bf16)
    rest_decay = (decay - near_decay.astype(f32)).astype(bf16)
    row8 = lax.broadcasted_iota(jnp.int32, (8, 128), 0)
    ssend[64:72, :] = jnp.where(
        row8 == 0, near_decay.astype(f32), jnp.where(row8 == 1, rest_decay.astype(f32), 0.0)
    ).astype(bf16)
    s_cp = [
        push(ssend, sst.at[ep], ss_s.at[d], sr_s.at[d], ep_at(d, 1), tp) for d in range(1, NEP)
    ]
    for cp in s_cp:
        cp.start()
    w_step(2, 1)


    def mixer_rest():
        for cp in s_cp:
            cp.wait_recv()

        def chain(j, ent):
            got = sst[j].astype(f32)
            return jnp.where(j < ep, ent * (got[64:65, :] + got[65:66, :]) + got[0:64, :], ent)

        ent = lax.fori_loop(0, NEP - 1, chain, jnp.zeros((64, 128), f32))
        entb[...] = jnp.zeros_like(entb)
        entb[half_rows, :] = ent.astype(bf16)
        scale = jnp.where(lane1 < 64, direct[0], direct[1])
        gain = gn[...].astype(f32)

        def rows_of(j, keep):
            for k in range(2):
                b = 2 * j + k
                rows = pl.ds(pl.multiple_of(b * 128, 128), 128)
                since_b = jnp.where(first, c0l[rows, :], c1l[rows, :]) + tst[pl.ds(b, 1), :]
                far = jnp.dot(csb[rows, :], entb[...], preferred_element_type=f32) * jnp.exp(since_b)
                gate = ogb[rows, :].astype(f32)
                val = (ssm[rows, :] + far + scale * xsb[rows, :].astype(f32)) * (gate * jax.nn.sigmoid(gate))
                sq = val * val
                sum0 = jnp.sum(jnp.where(first, sq, 0.0), axis=1, keepdims=True)
                sum1 = jnp.sum(jnp.where(first, 0.0, sq), axis=1, keepdims=True)
                ms = jnp.where(first, sum0, sum1) * (1.0 / 64)
                keep(k, rows, (val * lax.rsqrt(ms + eps) * gain).astype(bf16))

        def send_on(i, _):
            j = (z + 1 + i) % NZ

            def keep(k, rows, val):
                mixb[rows, :] = val

            rows_of(j, keep)
            push(
                mixb.at[pl.ds(pl.multiple_of(j * 256, 256), 256), :],
                mx.at[:, pl.ds(pl.multiple_of((7 - i) * 128, 128), 128)],
                ms_s.at[7 - i], mr_s.at[7 - i], ep, tp_at(1 + i),
            ).start()
            return 0

        lax.fori_loop(0, NZ - 1, send_on, 0)

        def own(k, rows, val):
            mx[128 * k : 128 * (k + 1), 0:128] = val

        rows_of(z, own)

    m_cp = [
        push(
            mixb.at[pl.ds(pl.multiple_of(((z + r) % NZ) * 256, 256), 256), :],
            mx.at[:, pl.ds((NZ - r) * 128, 128)],
            ms_s.at[NZ - r], mr_s.at[NZ - r], ep, tp_at(r),
        )
        for r in range(1, NZ)
    ]

    lg.wait()
    lu.wait()
    for cp in dn_l:
        cp.wait()

    def y_copy(d, h):
        part = (pl.ds(d * CAP, CAP), pl.ds(h * 512, 512))
        return push(ysend.at[part], ybuf.at[part], ys_s.at[h, d], yr_s.at[h, d], ep_at(d, -1), tp)

    y_cp = [[y_copy(d, h) for d in range(1, NEP)] for h in range(2)]
    h_cp = []
    for g in range(4):
        part = hall.at[c, pl.ds(256 * g, 256), :]
        h_cp.append(push(part, part, hs_s.at[g], hr_s.at[g], ep, other))

    def hidden(g):
        for d in range(4 * g, 4 * g + 4):
            hand[d].wait_recv()
        rows = slice(256 * g, 256 * (g + 1))
        xg = xr[rows, :]
        gv = jnp.dot(xg, gw[...], preferred_element_type=f32)
        uv = jnp.dot(xg, uw[...], preferred_element_type=f32)
        hall[c, rows, :] = (gv * jax.nn.sigmoid(gv) * uv).astype(bf16)
        h_cp[g].start()

    def results(g):
        rows = slice(256 * g, 256 * (g + 1))
        h_cp[g].wait_recv()
        yv = jnp.dot(hall[0, rows, :], dn[0], preferred_element_type=f32)
        yv += jnp.dot(hall[1, rows, :], dn[1], preferred_element_type=f32)
        ysend[rows, :] = yv.astype(bf16)
        for d in range(4 * g, 4 * g + 4):
            if d > 0:
                y_cp[0][d - 1].start()

    pass_on(0)
    pass_on(1)
    hidden(0)
    hidden(1)
    for cq in dn_r:
        cq.wait_recv()
    w_step(3, 0)
    results(0)
    results(1)
    w_step(3, 1)
    pass_on(2)
    hidden(2)
    pass_on(3)
    results(2)
    hidden(3)
    results(3)
    for d in range(1, NEP):
        y_cp[1][d - 1].start()
    w_step(4, 0)
    w_step(4, 1)
    mixer_rest()
    ybuf[0:CAP, :] = ysend[0:CAP, :]

    def project():
        lw.wait()
        for cp in m_cp:
            cp.wait_recv()
        for way in range(2):
            w_cp[way, 3, 1 - way].wait_recv()
            w_cp[way, 4, way].wait_recv()
        theirs = mx[pl.ds(pl.multiple_of((1 - c) * 128, 128), 128), :]
        psend[...] = jnp.dot(theirs, wg[...], preferred_element_type=f32).astype(bf16)
        fin = push(psend, precv, fs_s, fr_s, ep, other)
        fin.start()
        ours = mx[pl.ds(pl.multiple_of(c * 128, 128), 128), :]
        mine = jnp.dot(ours, wg[...], preferred_element_type=f32)
        keep_mine[...] = mine
        return fin

    first_hop = {4: (2, 0), 3: (1, 1), 5: (7, 2)}
    z_cp, on_way = [], []
    for h in range(2):
        for d in range(1, NEP):
            y_cp[h][d - 1].wait_recv()
        cols = slice(512 * h, 512 * (h + 1))
        comb = jnp.dot(mixw, ybuf[:, cols], preferred_element_type=f32)
        for i in ((0, 1, 2, 3), (2, 3, 0, 1))[h]:
            r = ORDER[4 * h + i]
            if r == 2:
                fin = project()
                for cp in on_way:
                    cp.wait_recv()
            val = comb[:, 128 * i : 128 * (i + 1)]
            if r == 0:
                zown[...] = val
                continue
            if r in first_hop:
                hop, place_w = first_hop[r]
                zsend[r] = val.astype(bf16)
                cp = push(zsend.at[r], zway.at[place_w], zws_s.at[place_w], zwr_s.at[place_w], ep, tp_at(hop))
                cp.start()
                on_way.append(cp)
                continue
            if r == 2:
                val = val + zway[0].astype(f32) + zway[1].astype(f32)
            if r == 6:
                val = val + zway[2].astype(f32)
            zsend[r] = val.astype(bf16)
            cp = push(zsend.at[r], zbuf.at[NZ - r], zs_s.at[NZ - r], zr_s.at[NZ - r], ep, tp_at(r))
            cp.start()
            z_cp.append(cp)

    fin.wait_recv()
    mo[...] = (keep_mine[...] + precv[...].astype(f32)).astype(bf16)

    acc = zown[...]
    for cp in z_cp:
        cp.wait_recv()
    for r in (1, 2, 6, 7):
        acc += zbuf[r].astype(f32)
    eo[...] = acc.astype(bf16)

    for cp in dn_r + m_cp + x_cp + halo + s_cp + hand + y_cp[0] + y_cp[1] + h_cp + z_cp + on_way + [fin]:
        cp.wait_send()
    for cp in w_cp.values():
        cp.wait_send()


def fused(*args):
    vmem, hbm = pl.BlockSpec(memory_space=pltpu.VMEM), pl.BlockSpec(memory_space=pl.ANY)
    smem = pl.BlockSpec(memory_space=pltpu.SMEM)
    dma = pltpu.SemaphoreType.DMA
    v = pltpu.VMEM
    return pl.pallas_call(
        kernel,
        out_shape=(
            pltpu.VMEM((128, 2048), bf16),
            pltpu.VMEM((256, 128), bf16),
        ),
        in_specs=[hbm] * 10 + [smem] * 2 + [hbm] * 9,
        out_specs=(vmem, vmem),
        scratch_shapes=[
            v((256, 2048), bf16),
            v((512, 2048), bf16),
            v((1024, 2048), bf16),
            v((2048, 256), bf16),
            v((2048, 256), bf16),
            v((2, 256, 1024), bf16),
            v((2, 1024, 256), bf16),
            v((1024, 1024), bf16),
            v((1024, 1024), bf16),
            v((8, 256, 128), bf16),
            v((8, 256, 128), bf16),
            v((1024, 2048), bf16),
            v((256, 1024), bf16),
            v((128, 2048), bf16),
            v((128, 2048), bf16),
            v((2056, 128), bf16),
            v((2056, 128), bf16),
            v((2056, 128), bf16),
            v((2048, 128), bf16),
            v((2048, 128), bf16),
            v((2048, 128), bf16),
            v((2048, 128), f32),
            v((2048, 128), f32),
            v((2048, 128), f32),
            v((32, 128), f32),
            v((32, 128), f32),
            v((16, 128), f32),
            v((2048, 128), f32),
            v((128, 128), f32),
            v((72, 128), bf16),
            v((16, 72, 128), bf16),
            v((128, 128), bf16),
            v((2048, 128), bf16),
            v((128, 2048), f32),
            v((256, 2048), bf16),
            v((3, 256, 128), bf16),
            v((256, 128), f32),
            v((16, 128), bf16),
            v((4, 2048), bf16),
            v((16, 2048), bf16),
            v((2, 256), jnp.int32),
            v((4, 128), bf16),
            v((4, 256), bf16),
            v((4, 256), bf16),
            v((32, 128), f32),
            v((32, 128), f32),
            v((1, 128), bf16),
            dma((10,)),
            dma((4,)),
            dma((8,)), dma((8,)), dma((8,)), dma((8,)),
            dma((16,)), dma((16,)), dma((16,)), dma((16,)),
            dma((4,)), dma((4,)), dma((2, 16)), dma((2, 16)),
            dma((8,)), dma((8,)), dma((2, 2, 4)), dma((2, 2, 4)), dma((8,)), dma((8,)),
            dma, dma, dma((3,)), dma((3,)), dma((16,)), dma((16,)),
            dma((3,)), dma((3,)),
        ],
        compiler_params=pltpu.CompilerParams(
            collective_id=0, has_side_effects=True, vmem_limit_bytes=56 * 1024 * 1024
        ),
    )(*args)


def per_device(
    mixer_input_channels,
    output_gate_logits,
    head_group_input_map,
    head_group_output_map,
    input_channel_taps,
    input_map_taps,
    output_map_taps,
    step_logits,
    head_log_rate,
    extra_log_decay,
    head_direct_scale,
    gated_norm_scale,
    mixer_output_weight,
    second_batch_tokens,
    pre_expert_norm_scale,
    group_router_columns,
    expert_router_columns,
    routes,
    expert_gate_weight,
    expert_up_weight,
    expert_down_weight,
):
    def by_block(v):
        return jnp.transpose(v.reshape(2, 16, 128), (1, 0, 2)).reshape(32, 128)

    return fused(
        pre_expert_norm_scale.reshape(16, 128),
        group_router_columns.T,
        expert_router_columns.T,
        routes.T,
        input_channel_taps,
        input_map_taps,
        output_map_taps,
        by_block(step_logits),
        by_block(extra_log_decay),
        gated_norm_scale.reshape(1, -1),
        head_log_rate,
        head_direct_scale,
        second_batch_tokens,
        expert_gate_weight[0],
        expert_up_weight[0],
        expert_down_weight[0],
        mixer_output_weight,
        mixer_input_channels,
        output_gate_logits,
        head_group_input_map,
        head_group_output_map,
    )


def solution(mesh):
    in_specs = (
        P("ep", "tp"),
        P("ep", "tp"),
        P("ep", None),
        P("ep", None),
        P(None, "tp"),
        P(),
        P(),
        P("tp", "ep"),
        P("tp"),
        P("tp", "ep"),
        P("tp"),
        P("tp"),
        P("tp", None),
        P("ep", None),
        P(),
        P(),
        P(),
        P("ep", None),
        P("ep", None, "tp"),
        P("ep", None, "tp"),
        P("ep", "tp", None),
    )
    out_specs = (P(("ep", "tp"), None), P("ep", "tp"))
    return jax.shard_map(
        per_device, mesh=mesh, in_specs=in_specs, out_specs=out_specs, check_vma=False
    )
```
